512 devices in a mesh: sp: 128 (over z, x, core), tp: 4 (over y).
Axes of the slice: x: 4, y: 4, z: 16, core: 2. Of those that a mesh axis runs over, the one named last changes fastest.
Arguments:
- inputs: bfloat16 [32768, 2048], P('sp', 'tp'), may hold values from -120 to 120
- in_gain: float32 [2048], replicated, may hold values from 0.1 to 1.9
- query_weight: bfloat16 [2048, 1024], P('sp', 'tp'), may hold values from -0.125 to 0.125
- key_weight: bfloat16 [2048, 1024], P('sp', 'tp'), may hold values from -0.125 to 0.125
- value_weight: bfloat16 [2048, 1024], P('sp', 'tp'), may hold values from -0.125 to 0.125
- beta_weight: bfloat16 [2, 2048, 8], replicated, may hold values from -0.125 to 0.125
- decay_weight: bfloat16 [2, 2048, 8], replicated, may hold values from -0.125 to 0.125
- beta_shift: float32 [2, 8], replicated, may hold values from -9 to 1
- decay_pace: float32 [2, 8, 32768], P(None, 'tp', 'sp'), may hold values from 0 to 0.1
- decay_jolt: float32 [2, 8, 32768], P(None, 'tp', 'sp'), may hold values from -1.4 to 0, as said below
- head_gain: float32 [128], replicated, may hold values from 0.1 to 1.9
- glu_value_weight: bfloat16 [2048, 1024], P('sp', 'tp'), may hold values from -0.125 to 0.125
- glu_gate_weight: bfloat16 [2048, 1024], P('sp', 'tp'), may hold values from -0.125 to 0.125
- conv_kernel: bfloat16 [31, 1024], P(None, 'tp'), may hold values from -4 to 4
- conv_gain: float32 [1024], P('tp'), may hold values from 0.1 to 1.9
- out_delta_weight: bfloat16 [1024, 2048], P('tp', 'sp'), may hold values from -0.125 to 0.125
- out_conv_weight: bfloat16 [1024, 2048], P('tp', 'sp'), may hold values from -0.125 to 0.125
Outputs:
- mixed: bfloat16 [32768, 2048], P(('sp', 'tp'))
The draws below stay inside these ranges and needn't reach their ends.
Inputs may be any that keep to these rules, and one draw needn't show every extreme that they name: `decay_jolt`: zero but at a few positions of each direction and head.
All inputs are finite; a program needn't handle non-finite values.
Results may differ from the reference program's by a relative error of at most 0.017.
Values may be sent and summed in bfloat16 or wider, within the bound.
A program may use at most 128 MiB of HBM per device.

```python
import math
import jax
import jax.numpy as jnp
from jax import lax

D = 2048
HEAD = 128
QK_HEADS = 8
V_HEADS = 8
CONV_CH = 1024
KERNEL = 31
BLOCK = 64
T_DEV = 256
SEQ = 32768
N_TP = 4


def slow_flags(key):
    slow_share = 0.5
    return jax.random.uniform(jax.random.fold_in(key, 41), (2, V_HEADS, 1), jnp.float32) < slow_share


def draw_inputs(key, part):
    row_scale = jnp.exp(jax.random.uniform(jax.random.fold_in(key, 2), (SEQ, 1), jnp.float32, 0.0, math.log(10.0)))
    column_scale = jnp.exp(jax.random.uniform(jax.random.fold_in(key, 3), (1, D), jnp.float32, 0.0, math.log(3.0)))
    base_draw = jnp.clip(jax.random.normal(jax.random.fold_in(key, 1), (SEQ, D), jnp.float32), -4.0, 4.0)
    return (base_draw * row_scale * column_scale).astype(jnp.bfloat16)


def draw_beta_shift(key, part):
    slow_heads = slow_flags(key)[:, :, 0]
    fast_shift = jax.random.uniform(jax.random.fold_in(key, 42), (2, V_HEADS), jnp.float32, -1.0, 1.0)
    strength = jnp.exp(jax.random.uniform(jax.random.fold_in(key, 46), (2, V_HEADS), jnp.float32, math.log(0.2), math.log(0.5)))
    slow_shift = jnp.log(strength * HEAD / SEQ)
    return jnp.where(slow_heads, slow_shift, fast_shift)


def draw_decay_pace(key, part):
    slow_heads = slow_flags(key)
    fast_rate = jnp.exp(jax.random.uniform(jax.random.fold_in(key, 43), (2, V_HEADS, 1), jnp.float32, math.log(0.015), math.log(0.05)))
    slow_rate = jnp.exp(jax.random.uniform(jax.random.fold_in(key, 44), (2, V_HEADS, 1), jnp.float32, math.log(0.2), math.log(0.6))) / SEQ
    factor = jnp.exp(jax.random.uniform(jax.random.fold_in(key, 45), (2, V_HEADS, SEQ // T_DEV, 1), jnp.float32, math.log(0.5), math.log(2.0)))
    factor = jnp.broadcast_to(factor, (2, V_HEADS, SEQ // T_DEV, T_DEV)).reshape(2, V_HEADS, SEQ)
    return jnp.where(slow_heads, slow_rate, fast_rate) * factor


def draw_decay_jolt(key, part):
    places = jax.random.randint(jax.random.fold_in(key, 51), (2, V_HEADS, 2, 1), 0, SEQ)
    depth = jnp.log(jax.random.uniform(jax.random.fold_in(key, 52), (2, V_HEADS, 2, 1), jnp.float32, 0.5, 0.8))
    position = jnp.arange(SEQ, dtype=jnp.int32)
    return jnp.sum(jnp.where(position[None, None, None, :] == places, depth, 0.0), axis=2)


def draw_conv_kernel(key, part):
    channel = jnp.arange(CONV_CH, dtype=jnp.float32) / max(CONV_CH - 1, 1)
    rise_factor = 3.0
    scale = jnp.exp(math.log(rise_factor) * channel) * (0.6 / math.sqrt(KERNEL))
    base_draw = jnp.clip(jax.random.normal(jax.random.fold_in(key, 62), (KERNEL, CONV_CH), jnp.float32), -4.0, 4.0)
    return (base_draw * scale[None, :]).astype(jnp.bfloat16)


def block_levels(own_key, dims, split, low, top_value):
    factor_of, own = 1.0, jax.random.fold_in(own_key, 6)
    for dim, shards_of in split:
        heights = jnp.exp(jax.random.uniform(jax.random.fold_in(own, dim), (shards_of,), jnp.float32, low / len(split), top_value / len(split)))
        factor_of = factor_of * jnp.repeat(heights, dims[dim] // shards_of).reshape([-1 if axis == dim else 1 for axis in range(len(dims))])
    return factor_of


def noise(key, dims, width, most, shards=(), kind=jnp.bfloat16):
    level = block_levels(key, dims, shards, -0.22, 0.18) if shards else 1.0
    entries = jax.random.normal(key, dims, jnp.float32) * width * level
    return jnp.minimum(jnp.maximum(entries, -most), most).astype(kind)


def setup_inputs(seed: int = 0) -> dict:
    streams_of = jax.random.split(jax.random.key(seed), 18)
    inputs = draw_inputs(jax.random.fold_in(streams_of[17], 71), 0)
    in_gain = jnp.clip(1.0 + 0.18 * jax.random.normal(streams_of[1], (D,), jnp.float32), 0.1, 1.9)
    query_weight = noise(streams_of[2], (D, QK_HEADS * HEAD), D ** -0.5, 0.125, ((0, 128), (1, 4)))
    key_weight = noise(streams_of[3], (D, QK_HEADS * HEAD), D ** -0.5, 0.125, ((0, 128), (1, 4)))
    value_weight = noise(streams_of[4], (D, V_HEADS * HEAD), D ** -0.5, 0.125, ((0, 128), (1, 4)))
    beta_weight = noise(streams_of[5], (2, D, V_HEADS), D ** -0.5, 0.125)
    decay_weight = noise(streams_of[6], (2, D, V_HEADS), D ** -0.5, 0.125)
    beta_shift = draw_beta_shift(jax.random.fold_in(streams_of[17], 71), 0)
    decay_pace = draw_decay_pace(jax.random.fold_in(streams_of[17], 71), 0)
    decay_jolt = draw_decay_jolt(jax.random.fold_in(streams_of[17], 71), 0)
    head_gain = jnp.clip(1.0 + 0.18 * jax.random.normal(streams_of[10], (HEAD,), jnp.float32), 0.1, 1.9)
    glu_value_weight = noise(streams_of[11], (D, CONV_CH), D ** -0.5, 0.125, ((0, 128), (1, 4)))
    glu_gate_weight = noise(streams_of[12], (D, CONV_CH), D ** -0.5, 0.125, ((0, 128), (1, 4)))
    conv_kernel = draw_conv_kernel(jax.random.fold_in(streams_of[17], 71), 0)
    conv_gain = jnp.clip(1.0 + 0.18 * jax.random.normal(streams_of[14], (CONV_CH,), jnp.float32), 0.1, 1.9)
    out_delta_weight = noise(streams_of[15], (V_HEADS * HEAD, D), (V_HEADS * HEAD + CONV_CH) ** -0.5, 0.125, ((0, 4), (1, 128)))
    out_conv_weight = noise(streams_of[16], (CONV_CH, D), (V_HEADS * HEAD + CONV_CH) ** -0.5, 0.125, ((0, 4), (1, 128)))
    return {"inputs": inputs, "in_gain": in_gain, "query_weight": query_weight, "key_weight": key_weight, "value_weight": value_weight, "beta_weight": beta_weight, "decay_weight": decay_weight, "beta_shift": beta_shift, "decay_pace": decay_pace, "decay_jolt": decay_jolt, "head_gain": head_gain, "glu_value_weight": glu_value_weight, "glu_gate_weight": glu_gate_weight, "conv_kernel": conv_kernel, "conv_gain": conv_gain, "out_delta_weight": out_delta_weight, "out_conv_weight": out_conv_weight}


highest = lax.Precision.HIGHEST

def matmul_high(left_side, right_side):
    return jnp.matmul(left_side, right_side, precision=highest)

def unit_lower_inverse(matrix):
    order_size = matrix.shape[-1]
    leading = matrix.shape[:-2]
    inverse = jnp.ones(leading + (order_size, 1, 1), jnp.float32)
    size_now = 1
    while size_now < order_size:
        pair_count = order_size // (2 * size_now)
        halves = inverse.reshape(leading + (pair_count, 2, size_now, size_now))
        upper_inv = halves[..., 0, :, :]
        lower_inv = halves[..., 1, :, :]
        block_grid = matrix.reshape(leading + (pair_count, 2 * size_now, pair_count, 2 * size_now))
        diagonal = jnp.moveaxis(jnp.diagonal(block_grid, axis1=-4, axis2=-2), -1, -3)
        corner = diagonal[..., size_now:, :size_now]
        below = -matmul_high(lower_inv, matmul_high(corner, upper_inv))
        top_half = jnp.concatenate([upper_inv, jnp.zeros_like(below)], axis=-1)
        bottom_half = jnp.concatenate([below, lower_inv], axis=-1)
        inverse = jnp.concatenate([top_half, bottom_half], axis=-2)
        size_now = 2 * size_now
    return inverse.reshape(leading + (order_size, order_size))

def block_terms(queries, key_rows, values, beta_gate, log_decay):
    span = key_rows.shape[-2]
    cumulative = jnp.cumsum(log_decay, axis=-1)
    lower_mask = jnp.tril(jnp.ones((span, span), dtype=bool))
    strict = jnp.tril(jnp.ones((span, span), dtype=bool), -1)
    log_gap = cumulative[..., :, None] - cumulative[..., None, :]
    decay_mask = jnp.where(lower_mask, jnp.exp(jnp.where(lower_mask, log_gap, 0.0)), 0.0)
    key_inner = matmul_high(key_rows, jnp.swapaxes(key_rows, -1, -2))
    below_part = jnp.where(strict, beta_gate[..., :, None] * key_inner * decay_mask, 0.0)
    inverse = unit_lower_inverse(below_part + jnp.eye(span, dtype=jnp.float32))
    fresh = matmul_high(inverse, values * beta_gate[..., None])
    weighted = matmul_high(inverse, key_rows * (beta_gate * jnp.exp(cumulative))[..., None])
    scores = matmul_high(queries, jnp.swapaxes(key_rows, -1, -2)) * decay_mask
    readout = queries * jnp.exp(cumulative)[..., None] - matmul_high(scores, weighted)
    tail_keys = jnp.swapaxes(key_rows * jnp.exp(cumulative[..., -1:] - cumulative)[..., None], -1, -2)
    identity = jnp.eye(key_rows.shape[-1], dtype=jnp.float32)
    carry_map = jnp.exp(cumulative[..., -1])[..., None, None] * identity - matmul_high(tail_keys, weighted)
    carry_add = matmul_high(tail_keys, fresh)
    within = matmul_high(scores, fresh)
    return (carry_map, carry_add, readout, within)

def layer_norm_rows(inputs, gain):
    as_float = inputs.astype(jnp.float32)
    mean_row = lax.optimization_barrier(jnp.mean(as_float, axis=-1, keepdims=True))
    spread = lax.optimization_barrier(jnp.mean(jnp.square(as_float - mean_row), axis=-1, keepdims=True))
    return ((as_float - mean_row) * lax.rsqrt(spread + 1e-05) * gain).astype(jnp.bfloat16)

def to_blocks(tensor):
    return tensor.reshape((tensor.shape[0] // BLOCK, BLOCK) + tensor.shape[1:])

def one_direction(queries, key_rows, values, beta_gate, log_decay):
    carry_map, carry_add, readout, within = block_terms(to_blocks(queries), to_blocks(key_rows), to_blocks(values), to_blocks(beta_gate), to_blocks(log_decay))

    def advance(carried, block_parts):
        step_map, step_add, step_read, step_within = block_parts
        return (matmul_high(step_map, carried) + step_add, matmul_high(step_read, carried) + step_within)
    initial = jnp.zeros((queries.shape[1], values.shape[1]), jnp.float32)
    _, outputs = lax.scan(advance, initial, (carry_map, carry_add, readout, within))
    return outputs.reshape(values.shape)

def reference(inputs, in_gain, query_weight, key_weight, value_weight, beta_weight, decay_weight, beta_shift, decay_pace, decay_jolt, head_gain, glu_value_weight, glu_gate_weight, conv_kernel, conv_gain, out_delta_weight, out_conv_weight):
    normed = layer_norm_rows(inputs, in_gain)
    queries = jnp.dot(normed, query_weight, preferred_element_type=jnp.float32).astype(jnp.bfloat16)
    key_proj = jnp.dot(normed, key_weight, preferred_element_type=jnp.float32).astype(jnp.bfloat16)
    value_proj = jnp.dot(normed, value_weight, preferred_element_type=jnp.float32).astype(jnp.bfloat16)
    glu_value = jnp.dot(normed, glu_value_weight, preferred_element_type=jnp.float32).astype(jnp.bfloat16)
    glu_gate = jnp.dot(normed, glu_gate_weight, preferred_element_type=jnp.float32).astype(jnp.bfloat16)
    beta_cols = jnp.moveaxis(beta_weight, 0, 1).reshape(D, 2 * V_HEADS)
    decay_cols = jnp.moveaxis(decay_weight, 0, 1).reshape(D, 2 * V_HEADS)
    beta_pre = jnp.transpose(jnp.dot(normed, beta_cols, preferred_element_type=jnp.float32).reshape(SEQ, 2, V_HEADS), (1, 2, 0))
    decay_pre = jnp.transpose(jnp.dot(normed, decay_cols, preferred_element_type=jnp.float32).reshape(SEQ, 2, V_HEADS), (1, 2, 0))
    beta_gate = jax.nn.sigmoid(beta_pre + beta_shift[:, :, None])
    log_decay = -decay_pace * jax.nn.softplus(decay_pre) + decay_jolt
    group_size = V_HEADS // QK_HEADS

    def head_output(head_index):
        key_start = head_index // group_size * HEAD
        q_head = jax.nn.silu(lax.dynamic_slice_in_dim(queries, key_start, HEAD, 1).astype(jnp.float32))
        k_head = jax.nn.silu(lax.dynamic_slice_in_dim(key_proj, key_start, HEAD, 1).astype(jnp.float32))
        k_head = k_head * lax.rsqrt(lax.optimization_barrier(jnp.sum(jnp.square(k_head), axis=-1, keepdims=True)) + 1e-06)
        v_head = lax.dynamic_slice_in_dim(value_proj, head_index * HEAD, HEAD, 1).astype(jnp.float32)
        gates = beta_gate[:, head_index]
        decays = log_decay[:, head_index]
        forward = one_direction(q_head, k_head, v_head, gates[0], decays[0])
        backward = jnp.flip(one_direction(jnp.flip(q_head, 0), jnp.flip(k_head, 0), jnp.flip(v_head, 0), jnp.flip(gates[1], 0), jnp.flip(decays[1], 0)), 0)
        combined = forward + backward
        scaled = combined * lax.rsqrt(lax.optimization_barrier(jnp.mean(jnp.square(combined), axis=-1, keepdims=True)) + 1e-06) * head_gain
        return scaled.astype(jnp.bfloat16)
    delta_heads = lax.map(head_output, jnp.arange(V_HEADS, dtype=jnp.int32))
    delta_out = jnp.transpose(delta_heads, (1, 0, 2)).reshape(SEQ, V_HEADS * HEAD)
    gated = (glu_value.astype(jnp.float32) * jax.nn.sigmoid(glu_gate.astype(jnp.float32))).astype(jnp.bfloat16)
    half_width = KERNEL // 2
    padded = jnp.pad(gated, ((half_width, half_width), (0, 0)))
    filtered = jnp.zeros((SEQ, CONV_CH), jnp.float32)
    for tap_index in range(KERNEL):
        filtered = filtered + padded[tap_index:tap_index + SEQ].astype(jnp.float32) * conv_kernel[tap_index].astype(jnp.float32)
    mean_row = lax.optimization_barrier(jnp.mean(filtered, axis=-1, keepdims=True))
    second = lax.optimization_barrier(jnp.mean(filtered * filtered, axis=-1, keepdims=True))
    conv_out = jax.nn.silu((filtered - mean_row) * lax.rsqrt(second - mean_row * mean_row + 1e-05) * conv_gain).astype(jnp.bfloat16)
    delta_group = V_HEADS * HEAD // N_TP
    conv_group = CONV_CH // N_TP
    totals = jnp.zeros((SEQ, D), jnp.float32)
    for group_index in range(N_TP):
        d_lo = group_index * delta_group
        c_lo = group_index * conv_group
        partial_value = jnp.dot(delta_out[:, d_lo:d_lo + delta_group], out_delta_weight[d_lo:d_lo + delta_group], preferred_element_type=jnp.float32)
        partial_value = partial_value + jnp.dot(conv_out[:, c_lo:c_lo + conv_group], out_conv_weight[c_lo:c_lo + conv_group], preferred_element_type=jnp.float32)
        totals = totals + partial_value.astype(jnp.bfloat16).astype(jnp.float32)
    return totals.astype(jnp.bfloat16)
```

```python
import jax
import jax.numpy as jnp
from jax import lax
from jax.experimental import pallas as pl
from jax.experimental.pallas import tpu as pltpu
from jax.sharding import Mesh
from jax.sharding import PartitionSpec as P

HEAD = 128
V_HEADS = 8
CONV_CH = 1024
KERNEL = 31
SP = ("sp_0", "sp_1", "sp_2")
SP_TP = ("sp_0", "sp_1", "sp_2", "tp")
Z, X, C, Y = (16, 4, 2, 4)
ROWS = 256
WIDE = 256
F32 = jnp.float32
BF16 = jnp.bfloat16
HIGHEST = lax.Precision.HIGHEST
MESH = pl.DeviceIdType.MESH
VMEM = pl.BlockSpec(memory_space=pltpu.VMEM)
PACKET = 208


def place():
    return tuple(lax.axis_index(a) for a in SP_TP)


def remote(src, dst, send, recv, to):
    return pltpu.make_async_remote_copy(
        src_ref=src, dst_ref=dst, send_sem=send, recv_sem=recv, device_id=to, device_id_type=MESH
    )


def greet(peers):
    barrier = pltpu.get_barrier_semaphore()
    for peer in peers:
        pl.semaphore_signal(barrier, inc=1, device_id=peer, device_id_type=MESH)
    pl.semaphore_wait(barrier, len(peers))


def bdot(a, b, dims):
    return lax.dot_general(
        a.astype(BF16), b.astype(BF16), (dims, ((), ())), preferred_element_type=F32
    )


def fdot(a, b, dims):
    return lax.dot_general(a, b, (dims, ((), ())), precision=HIGHEST, preferred_element_type=F32)


def gather_kernel(w_ref, x_ref, g_ref, f_ref, zs, zr, xs, xr, ds, dr, ys, yr, own):
    z, x, c, y = place()
    zp, zm = (lax.rem(z + 1, Z), lax.rem(z + Z - 1, Z))
    xp, xm = (lax.rem(x + 1, X), lax.rem(x + X - 1, X))
    up, down = ((zp, x, c, y), (zm, x, c, y))
    right, left = ((z, xp, c, y), (z, xm, c, y))
    other = (z, x, 1 - c, y)
    mates = [(z, x, c, lax.rem(y + d, Y)) for d in (2, 1, 3)]

    greet([up, down, right, left, other] + mates)

    feature_copies = []
    for i, mate in enumerate(mates):
        copy = remote(x_ref, f_ref.at[y], ys.at[i], yr.at[i], mate)
        copy.start()
        feature_copies.append(copy)

    def chunk(zi, xi):
        return g_ref.at[:, zi, xi, c]

    def z_copy(src, zi, s, way, to):
        return remote(src, chunk(zi, x), zs.at[s, way], zr.at[s, way], to)

    def x_copy(src, zi, xi, s, way, to):
        return remote(src, chunk(zi, xi), xs.at[s, way], xr.at[s, way], to)

    def d_copy(zi, ci, s, way):
        line = g_ref.at[:, zi, :, ci]
        return remote(line, line, ds.at[s, way], dr.at[s, way], other)

    def behind(s):
        return lax.rem(z + Z - s, Z)

    def ahead(s):
        return lax.rem(z + s, Z)

    def z_start(s):
        p = chunk(behind(s), x)
        z_copy(p, behind(s), s, 0, up).wait_recv()

    def spread_p(s, src):
        x_copy(src, behind(s), x, s, 0, right).start()
        x_copy(src, behind(s), x, s, 1, left).start()

    def spread_q(s):
        src = chunk(ahead(s), x)
        x_copy(src, ahead(s), x, s, 2, left).start()
        x_copy(src, ahead(s), x, s, 3, right).start()

    def along_z(s, both, go_p, go_q):
        p, q = (chunk(behind(s), x), chunk(ahead(s), x))
        z_copy(p, behind(s), s, 0, up).wait_recv()
        if go_p:
            z_copy(p, behind(s), s + 1, 0, up).start()
        if both:
            z_copy(q, ahead(s), s, 1, down).wait_recv()
            if go_q:
                z_copy(q, ahead(s), s + 1, 1, down).start()
        spread_p(s, p)
        if both:
            spread_q(s)

    def forward(s, both):
        p = chunk(behind(s), xm)
        x_copy(p, behind(s), xm, s, 0, right).wait_recv()
        x_copy(p, behind(s), xm, s, 4, right).start()
        if both:
            q = chunk(ahead(s), xp)
            x_copy(q, ahead(s), xp, s, 2, left).wait_recv()
            x_copy(q, ahead(s), xp, s, 5, left).start()

    def across(s, both):
        far = lax.rem(x + 2, X)
        x_copy(chunk(behind(s), xp), behind(s), xp, s, 1, left).wait_recv()
        x_copy(chunk(behind(s), far), behind(s), far, s, 4, right).wait_recv()
        d_copy(behind(s), c, s, 0).start()
        if both:
            x_copy(chunk(ahead(s), xm), ahead(s), xm, s, 3, right).wait_recv()
            x_copy(chunk(ahead(s), far), ahead(s), far, s, 5, left).wait_recv()
            d_copy(ahead(s), c, s, 1).start()

    z_copy(w_ref, z, 1, 0, up).start()
    z_copy(w_ref, z, 1, 1, down).start()
    spread_p(0, w_ref)
    mine = pltpu.make_async_copy(w_ref, chunk(z, x), own.at[0])
    mine.start()
    keep = pltpu.make_async_copy(x_ref, f_ref.at[y], own.at[1])
    keep.start()
    mine.wait()
    along_z(1, True, True, True)
    forward(0, False)
    along_z(2, True, True, True)
    forward(1, True)
    across(0, False)

    @pl.loop(3, 7)
    def _(s):
        along_z(s, True, True, True)
        forward(s - 1, True)
        across(s - 2, True)

    along_z(7, True, True, False)
    forward(6, True)
    across(5, True)
    along_z(8, False, False, False)
    forward(7, True)
    across(6, True)
    forward(8, False)
    across(7, True)
    across(8, False)

    def d_arrived(s, way):
        d_copy(behind(s) if way == 0 else ahead(s), 1 - c, s, way).wait_recv()

    def sent(s, both, zed):
        p, q = (chunk(behind(s), x), chunk(ahead(s), x))
        if zed:
            z_copy(p, behind(s), s, 0, up).wait_send()
            if both:
                z_copy(q, ahead(s), s, 1, down).wait_send()
        for way in (0, 1, 4) + ((2, 3, 5) if both else ()):
            x_copy(p, behind(s), x, s, way, right).wait_send()
        d_copy(behind(s), c, s, 0).wait_send()
        if both:
            d_copy(ahead(s), c, s, 1).wait_send()

    d_arrived(0, 0)
    sent(0, False, False)

    @pl.loop(1, 8)
    def _(s):
        d_arrived(s, 0)
        d_arrived(s, 1)
        sent(s, True, True)

    d_arrived(8, 0)
    sent(8, False, True)
    for i, copy in enumerate(feature_copies):
        copy.wait_send()
    for i, mate in enumerate(mates):
        src_y = lax.rem(y + Y - (2, 1, 3)[i], Y)
        remote(x_ref, f_ref.at[src_y], ys.at[i], yr.at[i], mate).wait_recv()
    keep.wait()


def gather_call(packed, features):
    count = packed.shape[0]
    dma = pltpu.SemaphoreType.DMA
    return pl.pallas_call(
        gather_kernel,
        out_shape=(
            jax.ShapeDtypeStruct((count, Z, X, C, 16, WIDE), BF16),
            jax.ShapeDtypeStruct((Y, ROWS, 512), BF16),
        ),
        in_specs=[VMEM] * 2,
        out_specs=(VMEM, VMEM),
        scratch_shapes=[
            dma((9, 2)), dma((9, 2)), dma((9, 6)), dma((9, 6)), dma((9, 2)), dma((9, 2)),
            dma((3,)), dma((3,)), dma((2,)),
        ],
        compiler_params=pltpu.CompilerParams(
            collective_id=0, has_side_effects=True, vmem_limit_bytes=40 * 2**20
        ),
        name="gather",
    )(packed, features)


def triangle(lower, strict):
    i = lax.broadcasted_iota(jnp.int32, (ROWS, ROWS), 0)
    j = lax.broadcasted_iota(jnp.int32, (ROWS, ROWS), 1)
    if lower:
        return i > j if strict else i >= j
    return i < j if strict else i <= j


def unit_inverse(below):
    i = lax.broadcasted_iota(jnp.int32, (ROWS, ROWS), 0)
    j = lax.broadcasted_iota(jnp.int32, (ROWS, ROWS), 1)
    eye = (i == j).astype(F32)
    size = 1
    inverse = None
    while size < ROWS:
        twice = 2 * size
        pair = ((i & -twice) == (j & -twice)) & ((i & size) != (j & size))
        corner = jnp.where(pair, below, 0.0)
        if inverse is None:
            inverse = eye - corner
        else:
            inner = bdot(corner, inverse, ((1,), (0,)))
            inverse = inverse - bdot(inverse, inner, ((1,), (0,)))
        size = twice
    low = (inverse - inverse.astype(BF16).astype(F32)).astype(BF16)
    high = inverse.astype(BF16)
    b_high = below.astype(BF16)
    b_low = (below - b_high.astype(F32)).astype(BF16)
    product = (
        bdot(b_high, high, ((1,), (0,)))
        + bdot(b_high, low, ((1,), (0,)))
        + bdot(b_low, high, ((1,), (0,)))
    )
    residual = eye - inverse - product
    return inverse + bdot(inverse, residual, ((1,), (0,)))


def silu(v):
    return v * jax.nn.sigmoid(v)


def local_kernel(
    f_ref, gain_ref, w_ref, gate_ref, shift_ref, pace_ref, jolt_ref,
    packet_ref, reach_ref, offset_ref, gated_ref, normed,
):
    total = jnp.zeros((ROWS, 1), F32)
    for p in range(Y):
        total = total + jnp.sum(f_ref[p].astype(F32), axis=1, keepdims=True)
    mean = total / 2048.0
    total = jnp.zeros((ROWS, 1), F32)
    for p in range(Y):
        total = total + jnp.sum(jnp.square(f_ref[p].astype(F32) - mean), axis=1, keepdims=True)
    scale = lax.rsqrt(total / 2048.0 + 1e-05)
    for p in range(Y):
        normed[:, p * 512 : (p + 1) * 512] = (
            (f_ref[p].astype(F32) - mean) * scale * gain_ref[p]
        ).astype(BF16)
    rows = normed[...]

    def project(k):
        return bdot(rows, w_ref[k], ((1,), (0,))).astype(BF16).astype(F32)

    gated_ref[...] = (project(3) * jax.nn.sigmoid(project(4))).astype(BF16)
    gates = bdot(gate_ref[...], rows, ((1,), (1,)))
    beta = jax.nn.sigmoid(gates[0:4] + shift_ref[...])
    pre = gates[4:8]
    soft = jnp.maximum(pre, 0.0) + jnp.log1p(jnp.exp(-jnp.abs(pre)))
    log_decay = -pace_ref[...] * soft + jolt_ref[...]
    upto = triangle(False, False).astype(F32)
    since = triangle(True, False).astype(F32)
    padded = jnp.concatenate([log_decay, jnp.zeros((4, ROWS), F32)], axis=0)
    ahead = fdot(padded, upto, ((1,), (0,)))
    back = fdot(padded, since, ((1,), (0,)))
    cumulative = jnp.concatenate([ahead[0:2], back[2:4]], axis=0)
    lines = jnp.concatenate([beta, cumulative], axis=0)
    columns = jnp.transpose(lines)

    query_all, key_all, value_all = (project(0), project(1), project(2))
    for h in range(2):
        lanes = slice(h * HEAD, (h + 1) * HEAD)
        q = silu(query_all[:, lanes])
        k = silu(key_all[:, lanes])
        k = k * lax.rsqrt(jnp.sum(jnp.square(k), axis=1, keepdims=True) + 1e-06)
        v = value_all[:, lanes]
        kk = bdot(k, k, ((1,), (1,)))
        qk = bdot(q, k, ((1,), (1,)))
        within = jnp.zeros((ROWS, HEAD), F32)
        for e in range(2):
            n = e * 2 + h
            b_col = columns[:, n : n + 1]
            c_col = columns[:, 4 + n : 5 + n]
            c_row = cumulative[n : n + 1, :]
            mask = triangle(e == 0, False)
            gap = jnp.where(mask, jnp.exp(jnp.where(mask, c_col - c_row, 0.0)), 0.0)
            below = jnp.where(triangle(e == 0, True), b_col * kk * gap, 0.0)
            inverse = unit_inverse(below)
            grown = jnp.exp(c_col)
            right = jnp.concatenate([v * b_col, k * (b_col * grown)], axis=1)
            both = bdot(inverse, right, ((1,), (0,)))
            read = bdot(qk * gap, both, ((1,), (0,)))
            within = within + read[:, :HEAD]
            reach_ref[e, h] = (q * grown - read[:, HEAD:]).astype(BF16)
            last = c_row[:, ROWS - 1 : ROWS] if e == 0 else c_row[:, 0:1]
            tail = k * jnp.exp(last - c_col)
            maps = bdot(both, tail, ((0,), (0,)))
            whole = jnp.broadcast_to(jnp.exp(last), (8, HEAD))
            high = whole.astype(BF16)
            low = (whole - high.astype(F32)).astype(BF16)
            for half in range(2):
                packet_ref[e, h, half, 0:128] = maps[128:256].astype(BF16)
                packet_ref[e, h, half, 128:192] = maps[half * 64 : half * 64 + 64].astype(BF16)
                packet_ref[e, h, half, 192:208] = jnp.concatenate(
                    [high.astype(F32), low.astype(F32)], axis=0
                ).astype(BF16)
        offset_ref[h] = within


def local_call(features, gain, weights, gates, shift, pace, jolt):
    return pl.pallas_call(
        local_kernel,
        out_shape=(
            jax.ShapeDtypeStruct((2, 2, 2, PACKET, HEAD), BF16),
            jax.ShapeDtypeStruct((2, 2, ROWS, HEAD), BF16),
            jax.ShapeDtypeStruct((2, ROWS, HEAD), F32),
            jax.ShapeDtypeStruct((ROWS, WIDE), BF16),
        ),
        in_specs=[VMEM] * 7,
        out_specs=(VMEM,) * 4,
        scratch_shapes=[pltpu.VMEM((ROWS, 2048), BF16)],
        compiler_params=pltpu.CompilerParams(vmem_limit_bytes=40 * 2**20),
        name="local",
    )(features, gain, weights, gates, shift, pace, jolt)


def unpack(ref, at):
    body = ref[at].astype(F32)
    return (body[0:192], body[192:193] + body[200:201])


def joined(first, second):
    (body1, a1), (body2, a2) = (first, second)
    turned = bdot(body1, body2[0:128], ((1,), (0,)))
    top = a1 * body2[0:128] + a2 * body1[0:128] - turned[0:128]
    bottom = a2 * body1[128:192] - turned[128:192] + body2[128:192]
    return (jnp.concatenate([top, bottom], axis=0), a1 * a2)


def carried_kernel(
    packet_ref, gated_ref, taps_ref, gain_ref, entry_ref, conv_ref,
    slab, before, leaving, near, far, parting, halo, stats, line, wide, filtered,
    ss, sr, ns, nr, fs, fr, es, er, hs, hr, ts, tr,
):
    z, x, c, y = place()
    step = 1 - 2 * c
    owner = c * X + x
    position = z * 8 + x * 2 + c
    mine = x * 2 + c

    def slab_peer(dx, dc):
        return (z, lax.rem(x + dx, X), c if dc == 0 else 1 - c, y)

    offsets = [(dx, dc) for dx in range(X) for dc in range(C) if (dx, dc) != (0, 0)]
    offsets = sorted(offsets, key=lambda o: -(2 if o[0] == 2 else min(o[0], 1)))
    mates = [(z, x, c, lax.rem(y + d, Y)) for d in (2, 1, 3)]

    def at_position(s):
        s = lax.rem(s + 128, 128)
        return (s // 8, lax.rem(s // 2, X), lax.rem(s, 2), y)

    following, preceding = (at_position(position + 1), at_position(position - 1))
    rest_of_z = [(lax.rem(z + d, Z), x, c, y) for d in range(1, Z)]

    near[...] = jnp.zeros_like(near)
    far[...] = jnp.zeros_like(far)
    greet([slab_peer(*o) for o in offsets] + mates + [following, preceding] + rest_of_z)

    slab_copies = []
    for i, (dx, dc) in enumerate(offsets):
        to = slab_peer(dx, dc)
        copy = remote(
            packet_ref.at[to[2] * X + to[1]], slab.at[mine], ss.at[i], sr.at[i], to
        )
        copy.start()
        slab_copies.append(copy)
    halo_copies = [
        remote(gated_ref.at[ROWS - 16 : ROWS], halo.at[0], hs.at[0], hr.at[0], following),
        remote(gated_ref.at[0:16], halo.at[1], hs.at[1], hr.at[1], preceding),
    ]
    for copy in halo_copies:
        copy.start()
    slab[mine] = packet_ref[owner]

    wide[16 : 16 + ROWS] = gated_ref[...].astype(F32)
    for copy in halo_copies:
        copy.wait_recv()
    wide[0:16] = halo[0].astype(F32) * (position > 0).astype(F32)
    wide[16 + ROWS : 32 + ROWS] = halo[1].astype(F32) * (position < 127).astype(F32)
    taps = taps_ref[...].astype(F32)

    @pl.loop(0, ROWS // 32)
    def _(r):
        window = wide[pl.ds(pl.multiple_of(r * 32, 32), 64)]
        total = jnp.zeros((32, WIDE), F32)
        for j in range(KERNEL):
            total = total + window[j + 1 : j + 33] * taps[j : j + 1]
        filtered[pl.ds(pl.multiple_of(r * 32, 32), 32)] = total

    ones = jnp.ones((8, WIDE), F32)
    whole = filtered[...]
    line[0:8] = fdot(ones, whole, ((1,), (1,)))
    line[8:16] = fdot(ones, whole * whole, ((1,), (1,)))
    stat_copies = []
    for i, mate in enumerate(mates):
        copy = remote(line, stats.at[i], ts.at[i], tr.at[i], mate)
        copy.start()
        stat_copies.append(copy)

    for i, (dx, dc) in enumerate(offsets):
        source = slab_peer(X - dx, dc)
        remote(
            packet_ref.at[owner], slab.at[source[1] * 2 + source[2]], ss.at[i], sr.at[i], source
        ).wait_recv()

    def nth(t):
        return jnp.where(c == 0, t, 7 - t)

    running = unpack(slab, nth(0))
    for t in range(1, 8):
        before[t, 0:192] = running[0].astype(BF16)
        before[t, 192:208] = jnp.broadcast_to(running[1], (16, HEAD)).astype(BF16)
        parting[t] = running[1]
        running = joined(running, unpack(slab, nth(t)))

    def pack(ref, value):
        body, a = value
        high = a.astype(BF16).astype(F32)
        ref[0:192] = body.astype(BF16)
        ref[192:208] = jnp.concatenate(
            [jnp.broadcast_to(high, (8, HEAD)), jnp.broadcast_to(a - high, (8, HEAD))], axis=0
        ).astype(BF16)

    def hop(d):
        return z + step * d

    def inside(d):
        return (hop(d) >= 0) & (hop(d) < Z)

    def z_peer(d):
        return (jnp.clip(hop(d), 0, Z - 1), x, c, y)

    def near_copy(i, d):
        return remote(leaving.at[0], near.at[i], ns.at[i], nr.at[i], z_peer(d))

    def far_copy(i, d):
        return remote(leaving.at[1], far.at[i], fs.at[i], fr.at[i], z_peer(d))

    pack(leaving.at[0], running)
    for i, d in ((2, 3), (1, 2), (0, 1)):

        @pl.when(inside(d))
        def _():
            near_copy(i, d).start()

    for copy in stat_copies:
        copy.wait_recv()
    summed = line[...] + stats[0] + stats[1] + stats[2]
    spread = jnp.full((8, WIDE), 0.125, F32)
    mean = fdot(summed[0:8], spread, ((0,), (0,))) / CONV_CH
    second = fdot(summed[8:16], spread, ((0,), (0,))) / CONV_CH
    conv_ref[...] = silu(
        (filtered[...] - mean) * lax.rsqrt(second - mean * mean + 1e-05) * gain_ref[...]
    ).astype(BF16)

    window = running
    for i, d in ((0, 1), (1, 2), (2, 3)):

        @pl.when(inside(-d))
        def _():
            near_copy(i, d).wait_recv()

        window = joined(unpack(near, i), window)
    pack(leaving.at[1], window)
    reaches = ((2, 9), (1, 5), (3, 13), (0, 1))
    for i, d in reaches:

        @pl.when(inside(d))
        def _():
            far_copy(i, d).start()

    @pl.when(inside(-1))
    def _():
        far_copy(0, 1).wait_recv()

    entering = unpack(far, 0)
    for i, d in ((1, 5), (2, 9), (3, 13)):

        @pl.when(inside(-d))
        def _():
            far_copy(i, d).wait_recv()

        entering = joined(unpack(far, i), entering)
    state = entering[0][128:192]
    line_up = [state]
    for t in range(1, 8):
        body = before[t].astype(F32)
        line_up.append(
            parting[t] * state - bdot(state, body[0:128], ((1,), (0,))) + body[128:192]
        )
    for t in range(8):
        slab[nth(t), 0:64] = line_up[t].astype(BF16)
    entry_ref[owner] = slab[mine, 0:64]
    entry_copies = []
    for i, (dx, dc) in enumerate(offsets):
        to = slab_peer(dx, dc)
        copy = remote(
            slab.at[to[1] * 2 + to[2], 0:64], entry_ref.at[owner], es.at[i], er.at[i], to
        )
        copy.start()
        entry_copies.append(copy)
    for i, (dx, dc) in enumerate(offsets):
        source = slab_peer(X - dx, dc)
        remote(
            slab.at[0, 0:64], entry_ref.at[source[2] * X + source[1]], es.at[i], er.at[i], source
        ).wait_recv()
    for copy in slab_copies + halo_copies + stat_copies + entry_copies:
        copy.wait_send()
    for i, d in ((0, 1), (1, 2), (2, 3)):

        @pl.when(inside(d))
        def _():
            near_copy(i, d).wait_send()

    for i, d in reaches:

        @pl.when(inside(d))
        def _():
            far_copy(i, d).wait_send()


def carried_call(packets, gated, taps, gain):
    dma = pltpu.SemaphoreType.DMA
    return pl.pallas_call(
        carried_kernel,
        out_shape=(
            jax.ShapeDtypeStruct((8, 64, HEAD), BF16),
            jax.ShapeDtypeStruct((ROWS, WIDE), BF16),
        ),
        in_specs=[VMEM] * 4,
        out_specs=(VMEM, VMEM),
        scratch_shapes=[
            pltpu.VMEM((8, PACKET, HEAD), BF16),
            pltpu.VMEM((8, PACKET, HEAD), BF16),
            pltpu.VMEM((2, PACKET, HEAD), BF16),
            pltpu.VMEM((3, PACKET, HEAD), BF16),
            pltpu.VMEM((4, PACKET, HEAD), BF16),
            pltpu.VMEM((8, 1, HEAD), F32),
            pltpu.VMEM((2, 16, WIDE), BF16),
            pltpu.VMEM((3, 16, WIDE), F32),
            pltpu.VMEM((16, WIDE), F32),
            pltpu.VMEM((ROWS + 64, WIDE), F32),
            pltpu.VMEM((ROWS, WIDE), F32),
            dma((7,)), dma((7,)), dma((3,)), dma((3,)), dma((4,)), dma((4,)),
            dma((7,)), dma((7,)), dma((2,)), dma((2,)), dma((3,)), dma((3,)),
        ],
        compiler_params=pltpu.CompilerParams(
            collective_id=1, has_side_effects=True, vmem_limit_bytes=40 * 2**20
        ),
        name="carried",
    )(packets, gated, taps, gain)


def final_kernel(
    entry_ref, reach_ref, offset_ref, conv_ref, gain_ref, w_ref, out_ref, parts, landed, s, r
):
    z, x, c, y = place()
    turns = (2, 1, 3)
    greet([(z, x, c, lax.rem(y + d, Y)) for d in turns])
    heads = []
    for h in range(2):
        o = offset_ref[h]
        for e in range(2):
            at = e * 4 + h * 2
            state = jnp.concatenate([entry_ref[at], entry_ref[at + 1]], axis=0)
            o = o + bdot(reach_ref[e, h], state, ((1,), (1,)))
        scale = lax.rsqrt(jnp.mean(jnp.square(o), axis=1, keepdims=True) + 1e-06)
        heads.append((o * scale * gain_ref[...]).astype(BF16))
    left = jnp.concatenate(heads, axis=1)
    total = bdot(left, w_ref[0], ((1,), (1,))) + bdot(conv_ref[...], w_ref[1], ((1,), (1,)))
    for p in range(Y):
        parts[p] = total[p * 64 : (p + 1) * 64].astype(BF16)
    copies = []
    for i, d in enumerate(turns):
        to = lax.rem(y + d, Y)
        copy = remote(parts.at[to], landed.at[i], s.at[i], r.at[i], (z, x, c, to))
        copy.start()
        copies.append(copy)
    result = parts[y].astype(F32)
    for i in (1, 2, 0):
        copies[i].wait_recv()
        result = result + landed[i].astype(F32)
    out_ref[...] = result.astype(BF16)
    for copy in copies:
        copy.wait_send()


def final_call(entry, reach, offset, conv_out, gain, weights):
    dma = pltpu.SemaphoreType.DMA
    return pl.pallas_call(
        final_kernel,
        out_shape=jax.ShapeDtypeStruct((64, 2048), BF16),
        in_specs=[VMEM] * 6,
        out_specs=VMEM,
        scratch_shapes=[
            pltpu.VMEM((Y, 64, 2048), BF16),
            pltpu.VMEM((3, 64, 2048), BF16),
            dma((3,)),
            dma((3,)),
        ],
        compiler_params=pltpu.CompilerParams(
            collective_id=2, has_side_effects=True, vmem_limit_bytes=40 * 2**20
        ),
        name="final",
    )(entry, reach, offset, conv_out, gain, weights)


def on_device(
    inputs,
    in_gain,
    query_weight,
    key_weight,
    value_weight,
    beta_weight,
    decay_weight,
    beta_shift,
    decay_pace,
    decay_jolt,
    head_gain,
    glu_value_weight,
    glu_gate_weight,
    conv_kernel,
    conv_gain,
    out_delta_weight,
    out_conv_weight,
):
    packed = jnp.stack(
        [
            query_weight,
            key_weight,
            value_weight,
            glu_value_weight,
            glu_gate_weight,
            out_delta_weight.T,
            out_conv_weight.T,
        ]
    )
    gathered, features = gather_call(packed, inputs)
    weights = gathered.reshape(7, 2048, WIDE)
    first = lax.axis_index("tp") * 2
    gates = jnp.stack([beta_weight, decay_weight])
    gates = lax.dynamic_slice_in_dim(gates, first, 2, 3)
    gates = jnp.transpose(gates, (0, 1, 3, 2)).reshape(8, 2048)
    shift = lax.dynamic_slice_in_dim(beta_shift, first, 2, 1).reshape(4, 1)
    packets, reach, offset, gated = local_call(
        features,
        in_gain.reshape(Y, 1, 512),
        weights[:5],
        gates,
        shift,
        decay_pace.reshape(4, ROWS),
        decay_jolt.reshape(4, ROWS),
    )
    entry, conv_out = carried_call(
        packets.reshape(8, PACKET, HEAD), gated, conv_kernel, conv_gain.reshape(1, WIDE)
    )
    return final_call(entry, reach, offset, conv_out, head_gain.reshape(1, HEAD), weights[5:])


def solution(mesh):
    finer = Mesh(mesh.devices.reshape(16, 4, 2, mesh.shape["tp"]), SP_TP)
    in_specs = (
        P(SP, "tp"),
        P(),
        P(SP, "tp"),
        P(SP, "tp"),
        P(SP, "tp"),
        P(),
        P(),
        P(),
        P(None, "tp", SP),
        P(None, "tp", SP),
        P(),
        P(SP, "tp"),
        P(SP, "tp"),
        P(None, "tp"),
        P("tp"),
        P("tp", SP),
        P("tp", SP),
    )
    return jax.shard_map(
        on_device, mesh=finer, in_specs=in_specs, out_specs=P(SP_TP, None), check_vma=False
    )
```

```python
import jax
import jax.numpy as jnp
from jax import lax
from jax.experimental import pallas as pl
from jax.experimental.pallas import tpu as pltpu
from jax.sharding import Mesh
from jax.sharding import PartitionSpec as P

HEAD = 128
V_HEADS = 8
CONV_CH = 1024
KERNEL = 31
SP = ("sp_0", "sp_1", "sp_2")
SP_TP = ("sp_0", "sp_1", "sp_2", "tp")
Z, X, C, Y = (16, 4, 2, 4)
ROWS = 256
WIDE = 256
F32 = jnp.float32
BF16 = jnp.bfloat16
HIGHEST = lax.Precision.HIGHEST
MESH = pl.DeviceIdType.MESH
VMEM = pl.BlockSpec(memory_space=pltpu.VMEM)
PACKET = 208


def place():
    return tuple(lax.axis_index(a) for a in SP_TP)


def remote(src, dst, send, recv, to):
    return pltpu.make_async_remote_copy(
        src_ref=src, dst_ref=dst, send_sem=send, recv_sem=recv, device_id=to, device_id_type=MESH
    )


def greet(peers):
    barrier = pltpu.get_barrier_semaphore()
    for peer in peers:
        pl.semaphore_signal(barrier, inc=1, device_id=peer, device_id_type=MESH)
    pl.semaphore_wait(barrier, len(peers))


def bdot(a, b, dims):
    return lax.dot_general(
        a.astype(BF16), b.astype(BF16), (dims, ((), ())), preferred_element_type=F32
    )


def fdot(a, b, dims):
    return lax.dot_general(a, b, (dims, ((), ())), precision=HIGHEST, preferred_element_type=F32)


def triangle(lower, strict):
    i = lax.broadcasted_iota(jnp.int32, (ROWS, ROWS), 0)
    j = lax.broadcasted_iota(jnp.int32, (ROWS, ROWS), 1)
    if lower:
        return i > j if strict else i >= j
    return i < j if strict else i <= j


def silu(v):
    return v * jax.nn.sigmoid(v)


def mixing_terms(k, q, v, kk, qk, b_col, c_col, c_row, lower):
    mask = triangle(lower, False)
    gap = jnp.where(mask, jnp.exp(jnp.where(mask, c_col - c_row, 0.0)), 0.0)
    below = jnp.where(triangle(lower, True), b_col * kk * gap, 0.0)
    return (qk * gap).astype(BF16), below


def grow_inverse(below, inverse, size):
    i = lax.broadcasted_iota(jnp.int32, (ROWS, ROWS), 0)
    j = lax.broadcasted_iota(jnp.int32, (ROWS, ROWS), 1)
    twice = 2 * size
    pair = ((i & -twice) == (j & -twice)) & ((i & size) != (j & size))
    corner = jnp.where(pair, below, 0.0).astype(BF16)
    if size == 1:
        return (i == j).astype(BF16) - corner
    inner = bdot(corner, inverse, ((1,), (0,)))
    return inverse - bdot(inverse, inner, ((1,), (0,))).astype(BF16)


def corrected_inverse(below, inverse):
    i = lax.broadcasted_iota(jnp.int32, (ROWS, ROWS), 0)
    j = lax.broadcasted_iota(jnp.int32, (ROWS, ROWS), 1)
    high = below.astype(BF16)
    low = (below - high.astype(F32)).astype(BF16)
    product = bdot(high, inverse, ((1,), (0,))) + bdot(low, inverse, ((1,), (0,)))
    wide = inverse.astype(F32)
    residual = (i == j).astype(F32) - wide - product
    return (wide + bdot(inverse, residual, ((1,), (0,)))).astype(BF16)


def unpack(ref, at):
    body = ref[at].astype(F32)
    return (body[0:192], body[192:193] + body[200:201])


def joined(first, second):
    (body1, a1), (body2, a2) = (first, second)
    turned = bdot(body1, body2[0:128], ((1,), (0,)))
    top = a1 * body2[0:128] + a2 * body1[0:128] - turned[0:128]
    bottom = a2 * body1[128:192] - turned[128:192] + body2[128:192]
    return (jnp.concatenate([top, bottom], axis=0), a1 * a2)


def layer_kernel(
    x_hbm, qw, kw, vw, gvw, ggw, odw, ocw, bw_hbm, dw_hbm, gain_hbm, shift_hbm, pace_hbm, jolt_hbm,
    taps_hbm, norm_hbm, head_hbm, out_ref,
    x_ref, mine, bw, dw, gain_ref, shift_ref, pace_ref, jolt_ref, taps_ref, norm_ref, head_ref,
    g1, g2, f_ref, gate_rows, normed, packet_ref, reach_ref, offset_ref, gated_ref,
    parts, landed, passing, entry_ref, conv_ref,
    slab, before, leaving, near, far, parting, halo, stats, line, wide, filtered,
    zs, zr, xs, xr, ds, dr, ys, yr, us, ur, vs, vr,
    ss, sr, ns, nr, fs, fr, es, er, hs, hr, ts, tr, ps, pr, own,
):
    fetches = [(x_hbm, x_ref)]
    fetches += [(ref, mine.at[n]) for n, ref in enumerate((qw, kw, vw, gvw, ggw, odw, ocw))]
    fetches += [(bw_hbm, bw), (dw_hbm, dw), (gain_hbm, gain_ref), (shift_hbm, shift_ref)]
    fetches += [(pace_hbm, pace_ref), (jolt_hbm, jolt_ref), (taps_hbm, taps_ref)]
    fetches += [(norm_hbm, norm_ref), (head_hbm, head_ref)]
    z, x, c, y = place()
    xp, xm = (lax.rem(x + 1, X), lax.rem(x + X - 1, X))
    opp = lax.rem(x + 2, X)
    right, left = ((z, xp, c, y), (z, xm, c, y))
    other = (z, x, 1 - c, y)
    mates = [(z, x, c, lax.rem(y + d, Y)) for d in (2, 1, 3)]

    def on_z(d):
        return (lax.rem(z + d + Z, Z), x, c, y)

    fetched = [pltpu.make_async_copy(*pair, own.at[3 + n]) for n, pair in enumerate(fetches)]
    for copy in fetched:
        copy.start()
    near[...] = jnp.zeros_like(near)
    far[...] = jnp.zeros_like(far)
    greet([on_z(1), on_z(-1), on_z(2), on_z(-2), right, left, other] + mates)
    for copy in fetched:
        copy.wait()

    groups = (g1, g2)
    own_rows = (mine.at[0:3], mine.at[3:7])

    def behind(s):
        return lax.rem(z + Z - s, Z)

    def ahead(s):
        return lax.rem(z + s, Z)

    def z_copy(g, src, zi, s, way, to):
        return remote(src, groups[g].at[:, zi, x, c], zs.at[g, s, way], zr.at[g, s, way], to)

    def z_in(g, s, way):
        zi = behind(s) if way == 0 else ahead(s)
        ref = groups[g].at[:, zi, x, c]
        z_copy(g, ref, zi, s, way, right).wait_recv()

    def z_on(g, s, way, d):
        zi = behind(s) if way == 0 else ahead(s)
        src = own_rows[g] if s == 0 else groups[g].at[:, zi, x, c]
        z_copy(g, src, zi, s + d, way, on_z(d if way == 0 else -d)).start()

    def chunk(zi, xi):
        return g1.at[:, zi, xi, c]

    def x_copy(src, zi, xi, s, way, to):
        return remote(src, chunk(zi, xi), xs.at[s, way], xr.at[s, way], to)

    def d_copy(zi, ci, s, way):
        line = g1.at[:, zi, :, ci]
        return remote(line, line, ds.at[s, way], dr.at[s, way], other)

    def spread_p(s, src):
        x_copy(src, behind(s), x, s, 0, right).start()
        x_copy(src, behind(s), x, s, 1, left).start()

    def spread_q(s):
        src = chunk(ahead(s), x)
        x_copy(src, ahead(s), x, s, 2, left).start()
        x_copy(src, ahead(s), x, s, 3, right).start()

    def forward(s, both):
        p = chunk(behind(s), xm)
        x_copy(p, behind(s), xm, s, 0, right).wait_recv()
        x_copy(p, behind(s), xm, s, 4, right).start()
        if both:
            q = chunk(ahead(s), xp)
            x_copy(q, ahead(s), xp, s, 2, left).wait_recv()
            x_copy(q, ahead(s), xp, s, 5, left).start()

    def across(s, both):
        x_copy(chunk(behind(s), xp), behind(s), xp, s, 1, left).wait_recv()
        x_copy(chunk(behind(s), opp), behind(s), opp, s, 4, right).wait_recv()
        d_copy(behind(s), c, s, 0).start()
        if both:
            x_copy(chunk(ahead(s), xm), ahead(s), xm, s, 3, right).wait_recv()
            x_copy(chunk(ahead(s), opp), ahead(s), opp, s, 5, left).wait_recv()
            d_copy(ahead(s), c, s, 1).start()

    for way in (0, 1):
        z_on(0, 0, way, 2)
        z_on(0, 0, way, 1)
    spread_p(0, own_rows[0])
    feature_copies = []
    for i, mate in enumerate(mates):
        copy = remote(x_ref, f_ref.at[y], ys.at[i], yr.at[i], mate)
        copy.start()
        feature_copies.append(copy)
    for way in (0, 1):
        z_on(1, 0, way, 2)
        z_on(1, 0, way, 1)
    keeps = [
        pltpu.make_async_copy(own_rows[0], g1.at[:, z, x, c], own.at[0]),
        pltpu.make_async_copy(own_rows[1], g2.at[:, z, x, c], own.at[1]),
        pltpu.make_async_copy(x_ref, f_ref.at[y], own.at[2]),
    ]
    for copy in keeps:
        copy.start()
    for copy in keeps:
        copy.wait()

    def z_round(r):
        s = 2 * r
        z_in(0, s, 0)
        if s < 8:
            z_on(0, s, 0, 2)
            z_on(0, s, 0, 1)
            z_in(0, s, 1)
            if s < 6:
                z_on(0, s, 1, 2)
            z_on(0, s, 1, 1)
        z_in(0, s - 1, 0)
        z_in(0, s - 1, 1)
        spread_p(s, chunk(behind(s), x))
        if s < 8:
            spread_q(s)
        spread_p(s - 1, chunk(behind(s - 1), x))
        spread_q(s - 1)

    def z_round_later(r):
        s = 2 * r
        z_in(1, s, 0)
        if s < 8:
            z_on(1, s, 0, 2)
            z_on(1, s, 0, 1)
            z_in(1, s, 1)
            if s < 6:
                z_on(1, s, 1, 2)
            z_on(1, s, 1, 1)
        z_in(1, s - 1, 0)
        z_in(1, s - 1, 1)

    z_round(1)
    forward(0, False)
    z_round_later(1)
    z_round(2)
    forward(2, True)
    forward(1, True)
    across(0, False)
    z_round_later(2)
    z_round(3)
    forward(4, True)
    forward(3, True)
    across(2, True)
    across(1, True)
    z_round_later(3)
    z_round(4)
    forward(6, True)
    forward(5, True)
    across(4, True)
    across(3, True)
    forward(8, False)
    forward(7, True)
    z_round_later(4)

    def column(n, xi, ci):
        return g2.at[2 * n : 2 * n + 2, :, xi, ci]

    def half_column(n, xi, k):
        return g2.at[2 * n : 2 * n + 2, 8 * k : 8 * k + 8, xi, c]

    def u_copy(n, xi, way, to):
        return remote(column(n, xi, c), column(n, xi, c), us.at[n, way], ur.at[n, way], to)

    def u_half(n, xi, way, to):
        line = half_column(n, xi, way)
        return remote(line, line, us.at[n, 2 + way], ur.at[n, 2 + way], to)

    def v_copy(n, xi, ci, k):
        return remote(column(n, xi, ci), column(n, xi, ci), vs.at[n, k], vr.at[n, k], other)

    def later_open(n):
        u_copy(n, x, 0, right).start()
        u_copy(n, x, 1, left).start()
        v_copy(n, x, c, 0).start()

    def later_turn(n):
        u_copy(n, xm, 0, right).wait_recv()
        u_half(n, xm, 0, right).start()
        u_copy(n, xp, 1, left).wait_recv()
        u_half(n, xp, 1, left).start()
        v_copy(n, xm, c, 1).start()
        v_copy(n, xp, c, 2).start()

    def later_close(n):
        u_half(n, opp, 0, right).wait_recv()
        u_half(n, opp, 1, left).wait_recv()
        v_copy(n, opp, c, 3).start()

    def later_end(n):
        for k, xi in enumerate((x, xm, xp, opp)):
            v_copy(n, xi, 1 - c, k).wait_recv()

    later_open(0)
    for i, mate in enumerate(mates):
        src_y = lax.rem(y + Y - (2, 1, 3)[i], Y)
        remote(x_ref, f_ref.at[src_y], ys.at[i], yr.at[i], mate).wait_recv()

    total = jnp.zeros((ROWS, 1), F32)
    for p in range(Y):
        total = total + jnp.sum(f_ref[p].astype(F32), axis=1, keepdims=True)
    mean = total / 2048.0
    total = jnp.zeros((ROWS, 1), F32)
    for p in range(Y):
        total = total + jnp.sum(jnp.square(f_ref[p].astype(F32) - mean), axis=1, keepdims=True)
    scale = lax.rsqrt(total / 2048.0 + 1e-05)
    for p in range(Y):
        normed[:, p * 512 : (p + 1) * 512] = (
            (f_ref[p].astype(F32) - mean) * scale * gain_ref[p]
        ).astype(BF16)
    across(6, True)
    across(5, True)
    across(8, False)
    across(7, True)
    i = lax.broadcasted_iota(jnp.int32, (V_HEADS, V_HEADS), 0)
    j = lax.broadcasted_iota(jnp.int32, (V_HEADS, V_HEADS), 1)
    eye = (i == j).astype(F32)
    turned_shift = fdot(eye, shift_ref[...], ((1,), (1,)))
    for e in range(2):
        for n, ref in ((e, bw), (2 + e, dw)):
            every_head = bdot(ref[e], normed[...], ((1,), (1,)))
            if n < 2:
                every_head = jax.nn.sigmoid(every_head + turned_shift[:, e : e + 1])
            for k in range(V_HEADS):
                gate_rows[n, k] = every_head[k : k + 1]
    first = y * 2

    def two_heads(n):
        return jnp.concatenate([gate_rows[n, first], gate_rows[n, first + 1]], axis=0)

    beta = jnp.concatenate([two_heads(0), two_heads(1)], axis=0)
    pre = jnp.concatenate([two_heads(2), two_heads(3)], axis=0)
    soft = jnp.maximum(pre, 0.0) + jnp.log1p(jnp.exp(-jnp.abs(pre)))
    pace = jnp.concatenate([pace_ref[0], pace_ref[1]], axis=0)
    jolt = jnp.concatenate([jolt_ref[0], jolt_ref[1]], axis=0)
    log_decay = -pace * soft + jolt
    upto = triangle(False, False).astype(F32)
    since = triangle(True, False).astype(F32)
    padded = jnp.concatenate([log_decay, jnp.zeros((4, ROWS), F32)], axis=0)
    forth = fdot(padded, upto, ((1,), (0,)))
    back = fdot(padded, since, ((1,), (0,)))
    cumulative = jnp.concatenate([forth[0:2], back[2:4]], axis=0)
    lines = jnp.concatenate([beta, cumulative], axis=0)
    columns = jnp.transpose(lines)

    def d_arrived(s, way):
        d_copy(behind(s) if way == 0 else ahead(s), 1 - c, s, way).wait_recv()

    d_arrived(0, 0)

    @pl.loop(1, 8)
    def _(s):
        d_arrived(s, 0)
        d_arrived(s, 1)

    d_arrived(8, 0)

    def project(ref, n):
        weight = ref[n].reshape(2048, WIDE)
        return bdot(normed[...], weight, ((1,), (0,))).astype(BF16).astype(F32)

    query_all, key_all, value_all = (project(g1, 0), project(g1, 1), project(g1, 2))
    chains = []
    for h in range(2):
        lanes = slice(h * HEAD, (h + 1) * HEAD)
        q = silu(query_all[:, lanes])
        k = silu(key_all[:, lanes])
        k = k * lax.rsqrt(jnp.sum(jnp.square(k), axis=1, keepdims=True) + 1e-06)
        v = value_all[:, lanes]
        kk = bdot(k, k, ((1,), (1,)))
        qk = bdot(q, k, ((1,), (1,)))
        for e in range(2):
            n = e * 2 + h
            b_col = columns[:, n : n + 1]
            c_col = columns[:, 4 + n : 5 + n]
            c_row = cumulative[n : n + 1, :]
            scores, below = mixing_terms(k, q, v, kk, qk, b_col, c_col, c_row, e == 0)
            chains.append((h, e, q, k, v, b_col, c_col, c_row, scores, below))
    inverses = [None] * 4
    size = 1
    while size < ROWS:
        inverses = [grow_inverse(t[9], inv, size) for t, inv in zip(chains, inverses)]
        size = 2 * size
        if size == 16:
            later_turn(0)
            later_open(1)
    inverses = [corrected_inverse(t[9], inv) for t, inv in zip(chains, inverses)]
    within = [jnp.zeros((ROWS, HEAD), F32)] * 2
    for (h, e, q, k, v, b_col, c_col, c_row, scores, below), inverse in zip(chains, inverses):
        grown = jnp.exp(c_col)
        rhs = jnp.concatenate([v * b_col, k * (b_col * grown)], axis=1)
        both = bdot(inverse, rhs, ((1,), (0,))).astype(BF16)
        read = bdot(scores, both, ((1,), (0,)))
        within[h] = within[h] + read[:, :HEAD]
        reach_ref[e, h] = (q * grown - read[:, HEAD:]).astype(BF16)
        last = c_row[:, ROWS - 1 : ROWS] if e == 0 else c_row[:, 0:1]
        tail = k * jnp.exp(last - c_col)
        maps = bdot(both, tail, ((0,), (0,)))
        whole = jnp.broadcast_to(jnp.exp(last), (8, HEAD))
        high = whole.astype(BF16).astype(F32)
        scalars = jnp.concatenate([high, whole - high], axis=0).astype(BF16)
        for half in range(2):
            n = e * 4 + h * 2 + half
            packet_ref[n, 0:128] = maps[128:256].astype(BF16)
            packet_ref[n, 128:192] = maps[half * 64 : half * 64 + 64].astype(BF16)
            packet_ref[n, 192:208] = scalars
    for h in range(2):
        offset_ref[h] = within[h]

    step = 1 - 2 * c
    owner = c * X + x
    position = z * 8 + x * 2 + c
    spot = x * 2 + c

    def slab_peer(dx, dc):
        return (z, lax.rem(x + dx, X), c if dc == 0 else 1 - c, y)

    offsets = [(dx, dc) for dx in range(X) for dc in range(C) if (dx, dc) != (0, 0)]
    offsets = sorted(offsets, key=lambda o: -(2 if o[0] == 2 else min(o[0], 1)))

    def at_position(s):
        s = lax.rem(s + 128, 128)
        return (s // 8, lax.rem(s // 2, X), lax.rem(s, 2), y)

    following, preceding = (at_position(position + 1), at_position(position - 1))
    slab_copies = []
    for i, (dx, dc) in enumerate(offsets):
        to = slab_peer(dx, dc)
        copy = remote(
            packet_ref.at[to[2] * X + to[1]], slab.at[spot], ss.at[i], sr.at[i], to
        )
        copy.start()
        slab_copies.append(copy)
    slab[spot] = packet_ref[owner]
    later_close(0)
    later_turn(1)
    later_end(0)
    gated_ref[...] = (project(g2, 0) * jax.nn.sigmoid(project(g2, 1))).astype(BF16)
    halo_copies = [
        remote(gated_ref.at[ROWS - 16 : ROWS], halo.at[0], hs.at[0], hr.at[0], following),
        remote(gated_ref.at[0:16], halo.at[1], hs.at[1], hr.at[1], preceding),
    ]
    for copy in halo_copies:
        copy.start()

    for i, (dx, dc) in enumerate(offsets):
        source = slab_peer(X - dx, dc)
        remote(
            packet_ref.at[owner], slab.at[source[1] * 2 + source[2]], ss.at[i], sr.at[i], source
        ).wait_recv()

    def nth(t):
        return jnp.where(c == 0, t, 7 - t)

    running = unpack(slab, nth(0))
    for t in range(1, 8):
        before[t, 0:192] = running[0].astype(BF16)
        parting[t] = running[1]
        running = joined(running, unpack(slab, nth(t)))

    def pack(ref, value):
        body, a = value
        high = a.astype(BF16).astype(F32)
        ref[0:192] = body.astype(BF16)
        ref[192:208] = jnp.concatenate(
            [jnp.broadcast_to(high, (8, HEAD)), jnp.broadcast_to(a - high, (8, HEAD))], axis=0
        ).astype(BF16)

    def hop(d):
        return z + step * d

    def inside(d):
        return (hop(d) >= 0) & (hop(d) < Z)

    def z_peer(d):
        return (jnp.clip(hop(d), 0, Z - 1), x, c, y)

    def near_copy(i, d):
        return remote(leaving.at[0], near.at[i], ns.at[i], nr.at[i], z_peer(d))

    def far_copy(i, d):
        return remote(leaving.at[1], far.at[i], fs.at[i], fr.at[i], z_peer(d))

    pack(leaving.at[0], running)
    for i, d in ((2, 3), (1, 2), (0, 1)):

        @pl.when(inside(d))
        def _():
            near_copy(i, d).start()

    wide[16 : 16 + ROWS] = gated_ref[...].astype(F32)
    for copy in halo_copies:
        copy.wait_recv()
    wide[0:16] = halo[0].astype(F32) * (position > 0).astype(F32)
    wide[16 + ROWS : 32 + ROWS] = halo[1].astype(F32) * (position < 127).astype(F32)
    taps = taps_ref[...].astype(F32)

    @pl.loop(0, ROWS // 32)
    def _(r):
        window = wide[pl.ds(pl.multiple_of(r * 32, 32), 64)]
        total = jnp.zeros((32, WIDE), F32)
        for j in range(KERNEL):
            total = total + window[j + 1 : j + 33] * taps[j : j + 1]
        filtered[pl.ds(pl.multiple_of(r * 32, 32), 32)] = total

    ones = jnp.ones((8, WIDE), F32)
    whole = filtered[...]
    line[0:8] = fdot(ones, whole, ((1,), (1,)))
    line[8:16] = fdot(ones, whole * whole, ((1,), (1,)))
    stat_copies = []
    for i, mate in enumerate(mates):
        copy = remote(line, stats.at[i], ts.at[i], tr.at[i], mate)
        copy.start()
        stat_copies.append(copy)

    window = running
    for i, d in ((0, 1), (1, 2), (2, 3)):

        @pl.when(inside(-d))
        def _():
            near_copy(i, d).wait_recv()

        window = joined(unpack(near, i), window)
    pack(leaving.at[1], window)
    reaches = ((2, 9), (1, 5), (3, 13), (0, 1))
    for i, d in reaches:

        @pl.when(inside(d))
        def _():
            far_copy(i, d).start()

    for copy in stat_copies:
        copy.wait_recv()
    summed = line[...] + stats[0] + stats[1] + stats[2]
    spread = jnp.full((8, WIDE), 0.125, F32)
    mean = fdot(summed[0:8], spread, ((0,), (0,))) / CONV_CH
    second = fdot(summed[8:16], spread, ((0,), (0,))) / CONV_CH
    conv_ref[...] = silu(
        (filtered[...] - mean) * lax.rsqrt(second - mean * mean + 1e-05) * norm_ref[...]
    ).astype(BF16)

    later_close(1)

    @pl.when(inside(-1))
    def _():
        far_copy(0, 1).wait_recv()

    entering = unpack(far, 0)
    for i, d in ((1, 5), (2, 9), (3, 13)):

        @pl.when(inside(-d))
        def _():
            far_copy(i, d).wait_recv()

        entering = joined(unpack(far, i), entering)
    state = entering[0][128:192]
    line_up = [state]
    for t in range(1, 8):
        body = before[t].astype(F32)
        line_up.append(
            parting[t] * state - bdot(state, body[0:128], ((1,), (0,))) + body[128:192]
        )
    for t in range(8):
        slab[nth(t), 0:64] = line_up[t].astype(BF16)
    entry_ref[owner] = slab[spot, 0:64]
    entry_copies = []
    for i, (dx, dc) in enumerate(offsets):
        to = slab_peer(dx, dc)
        copy = remote(
            slab.at[to[1] * 2 + to[2], 0:64], entry_ref.at[owner], es.at[i], er.at[i], to
        )
        copy.start()
        entry_copies.append(copy)
    for i, (dx, dc) in enumerate(offsets):
        source = slab_peer(X - dx, dc)
        remote(
            slab.at[0, 0:64], entry_ref.at[source[2] * X + source[1]], es.at[i], er.at[i], source
        ).wait_recv()
    later_end(1)
    heads = []
    for h in range(2):
        o = offset_ref[h]
        for e in range(2):
            at = e * 4 + h * 2
            state = jnp.concatenate([entry_ref[at], entry_ref[at + 1]], axis=0)
            o = o + bdot(reach_ref[e, h], state, ((1,), (1,)))
        scale = lax.rsqrt(jnp.mean(jnp.square(o), axis=1, keepdims=True) + 1e-06)
        heads.append((o * scale * head_ref[...]).astype(BF16))
    delta = jnp.concatenate(heads, axis=1)
    conv = conv_ref[...]
    beside, facing = (y + 1 - 2 * lax.rem(y, 2), 3 - y)
    opposite = lax.rem(y + 2, Y)
    ways = ((beside, facing), (facing, beside))
    for n in range(2):
        a = g2[2].reshape(2048, WIDE)[n * 1024 : (n + 1) * 1024]
        b = g2[3].reshape(2048, WIDE)[n * 1024 : (n + 1) * 1024]
        total = bdot(delta, a, ((1,), (1,))) + bdot(conv, b, ((1,), (1,)))
        for p in range(Y):
            parts[n, p] = total[p * 64 : (p + 1) * 64].astype(BF16)

    def part_copy(n, k, block):
        to = (z, x, c, ways[n][0])
        return remote(parts.at[n, block], landed.at[n, k], ps.at[n, k], pr.at[n, k], to)

    def pass_copy(n):
        to = (z, x, c, ways[n][1])
        return remote(passing.at[n], landed.at[n, 2], ps.at[n, 2], pr.at[n, 2], to)

    for n in range(2):
        part_copy(n, 0, opposite).start()
    for n in range(2):
        part_copy(n, 1, ways[n][0]).start()
    for n in range(2):
        part_copy(n, 0, opposite).wait_recv()
        passing[n] = (parts[n, ways[n][1]].astype(F32) + landed[n, 0].astype(F32)).astype(BF16)
        pass_copy(n).start()
    for n in range(2):
        part_copy(n, 1, y).wait_recv()
        pass_copy(n).wait_recv()
        out_ref[:, n * 1024 : (n + 1) * 1024] = (
            parts[n, y].astype(F32) + landed[n, 1].astype(F32) + landed[n, 2].astype(F32)
        ).astype(BF16)
    for n in range(2):
        part_copy(n, 0, opposite).wait_send()
        part_copy(n, 1, y).wait_send()
        pass_copy(n).wait_send()
    for copy in slab_copies + halo_copies + stat_copies + entry_copies:
        copy.wait_send()
    for i, d in ((0, 1), (1, 2), (2, 3)):

        @pl.when(inside(d))
        def _():
            near_copy(i, d).wait_send()

    for i, d in reaches:

        @pl.when(inside(d))
        def _():
            far_copy(i, d).wait_send()

    def sent(s, both, zed):
        p, q = (chunk(behind(s), x), chunk(ahead(s), x))
        for g in (0, 1) if zed else ():
            for way in (0, 1) if both else (0,):
                ref = groups[g].at[:, behind(s), x, c]
                z_copy(g, ref, behind(s), s, way, right).wait_send()
        for way in (0, 1, 4) + ((2, 3, 5) if both else ()):
            x_copy(p, behind(s), x, s, way, right).wait_send()
        d_copy(behind(s), c, s, 0).wait_send()
        if both:
            d_copy(ahead(s), c, s, 1).wait_send()

    sent(0, False, False)

    @pl.loop(1, 8)
    def _(s):
        sent(s, True, True)

    sent(8, False, True)
    for copy in feature_copies:
        copy.wait_send()
    for n in range(2):
        u_copy(n, x, 0, right).wait_send()
        u_copy(n, x, 1, left).wait_send()
        u_half(n, xm, 0, right).wait_send()
        u_half(n, xp, 1, left).wait_send()
        for k in range(4):
            v_copy(n, x, c, k).wait_send()


def layer_call(arrays):
    dma = pltpu.SemaphoreType.DMA
    anywhere = pl.BlockSpec(memory_space=pl.ANY)
    vmem = pltpu.VMEM
    return pl.pallas_call(
        layer_kernel,
        out_shape=jax.ShapeDtypeStruct((64, 2048), BF16),
        in_specs=[anywhere] * len(arrays),
        out_specs=VMEM,
        scratch_shapes=[
            vmem((ROWS, 512), BF16), vmem((7, 16, WIDE), BF16),
            vmem((2, V_HEADS, 2048), BF16), vmem((2, V_HEADS, 2048), BF16),
            vmem((Y, 1, 512), F32), vmem((2, V_HEADS), F32), vmem((2, 2, ROWS), F32),
            vmem((2, 2, ROWS), F32), vmem((KERNEL, WIDE), BF16), vmem((1, WIDE), F32),
            vmem((1, HEAD), F32),
            vmem((3, Z, X, C, 16, WIDE), BF16), vmem((4, Z, X, C, 16, WIDE), BF16),
            vmem((Y, ROWS, 512), BF16), vmem((4, V_HEADS, 1, ROWS), F32),
            vmem((ROWS, 2048), BF16),
            vmem((8, PACKET, HEAD), BF16), vmem((2, 2, ROWS, HEAD), BF16),
            vmem((2, ROWS, HEAD), F32), vmem((ROWS, WIDE), BF16),
            vmem((2, Y, 64, 1024), BF16), vmem((2, 3, 64, 1024), BF16), vmem((2, 64, 1024), BF16),
            vmem((8, 64, HEAD), BF16), vmem((ROWS, WIDE), BF16),
            vmem((8, PACKET, HEAD), BF16), vmem((8, PACKET, HEAD), BF16),
            vmem((2, PACKET, HEAD), BF16), vmem((3, PACKET, HEAD), BF16),
            vmem((4, PACKET, HEAD), BF16), vmem((8, 1, HEAD), F32), vmem((2, 16, WIDE), BF16),
            vmem((3, 16, WIDE), F32), vmem((16, WIDE), F32), vmem((ROWS + 64, WIDE), F32),
            vmem((ROWS, WIDE), F32),
            dma((2, 9, 2)), dma((2, 9, 2)), dma((9, 6)), dma((9, 6)), dma((9, 2)), dma((9, 2)),
            dma((3,)), dma((3,)), dma((2, 4)), dma((2, 4)), dma((2, 4)), dma((2, 4)),
            dma((7,)), dma((7,)), dma((3,)), dma((3,)), dma((4,)), dma((4,)),
            dma((7,)), dma((7,)), dma((2,)), dma((2,)), dma((3,)), dma((3,)),
            dma((2, 3)), dma((2, 3)), dma((3 + len(arrays),)),
        ],
        compiler_params=pltpu.CompilerParams(
            collective_id=0, has_side_effects=True, vmem_limit_bytes=63 * 2**20
        ),
        name="layer",
    )(*arrays)


def on_device(
    inputs,
    in_gain,
    query_weight,
    key_weight,
    value_weight,
    beta_weight,
    decay_weight,
    beta_shift,
    decay_pace,
    decay_jolt,
    head_gain,
    glu_value_weight,
    glu_gate_weight,
    conv_kernel,
    conv_gain,
    out_delta_weight,
    out_conv_weight,
):
    return layer_call(
        [
            inputs,
            query_weight,
            key_weight,
            value_weight,
            glu_value_weight,
            glu_gate_weight,
            out_delta_weight.T,
            out_conv_weight.T,
            jnp.transpose(beta_weight, (0, 2, 1)),
            jnp.transpose(decay_weight, (0, 2, 1)),
            in_gain.reshape(Y, 1, 512),
            beta_shift,
            decay_pace,
            decay_jolt,
            conv_kernel,
            conv_gain.reshape(1, WIDE),
            head_gain.reshape(1, HEAD),
        ]
    )


def solution(mesh):
    finer = Mesh(mesh.devices.reshape(16, 4, 2, mesh.shape["tp"]), SP_TP)
    in_specs = (
        P(SP, "tp"),
        P(),
        P(SP, "tp"),
        P(SP, "tp"),
        P(SP, "tp"),
        P(),
        P(),
        P(),
        P(None, "tp", SP),
        P(None, "tp", SP),
        P(),
        P(SP, "tp"),
        P(SP, "tp"),
        P(None, "tp"),
        P("tp"),
        P("tp", SP),
        P("tp", SP),
    )
    return jax.shard_map(
        on_device, mesh=finer, in_specs=in_specs, out_specs=P(SP_TP, None), check_vma=False
    )
```

```python
import jax
import jax.numpy as jnp
from jax import lax
from jax.experimental import pallas as pl
from jax.experimental.pallas import tpu as pltpu
from jax.sharding import Mesh
from jax.sharding import PartitionSpec as P

HEAD = 128
V_HEADS = 8
CONV_CH = 1024
KERNEL = 31
SP = ("sp_0", "sp_1", "sp_2")
SP_TP = ("sp_0", "sp_1", "sp_2", "tp")
Z, X, C, Y = (16, 4, 2, 4)
ROWS = 256
WIDE = 256
F32 = jnp.float32
BF16 = jnp.bfloat16
HIGHEST = lax.Precision.HIGHEST
MESH = pl.DeviceIdType.MESH
VMEM = pl.BlockSpec(memory_space=pltpu.VMEM)
PACKET = 208


def place():
    return tuple(lax.axis_index(a) for a in SP_TP)


def remote(src, dst, send, recv, to):
    return pltpu.make_async_remote_copy(
        src_ref=src, dst_ref=dst, send_sem=send, recv_sem=recv, device_id=to, device_id_type=MESH
    )


def greet(peers):
    barrier = pltpu.get_barrier_semaphore()
    for peer in peers:
        pl.semaphore_signal(barrier, inc=1, device_id=peer, device_id_type=MESH)
    pl.semaphore_wait(barrier, len(peers))


def bdot(a, b, dims):
    return lax.dot_general(
        a.astype(BF16), b.astype(BF16), (dims, ((), ())), preferred_element_type=F32
    )


def fdot(a, b, dims):
    return lax.dot_general(a, b, (dims, ((), ())), precision=HIGHEST, preferred_element_type=F32)


def triangle(lower, strict):
    i = lax.broadcasted_iota(jnp.int32, (ROWS, ROWS), 0)
    j = lax.broadcasted_iota(jnp.int32, (ROWS, ROWS), 1)
    if lower:
        return i > j if strict else i >= j
    return i < j if strict else i <= j


def silu(v):
    return v * jax.nn.sigmoid(v)


def mixing_terms(k, q, v, kk, qk, b_col, c_col, c_row, lower):
    mask = triangle(lower, False)
    gap = jnp.where(mask, jnp.exp(jnp.where(mask, c_col - c_row, 0.0)), 0.0)
    below = jnp.where(triangle(lower, True), b_col * kk * gap, 0.0)
    return (qk * gap).astype(BF16), below


def grow_inverse(below, inverse, size):
    i = lax.broadcasted_iota(jnp.int32, (ROWS, ROWS), 0)
    j = lax.broadcasted_iota(jnp.int32, (ROWS, ROWS), 1)
    twice = 2 * size
    pair = ((i & -twice) == (j & -twice)) & ((i & size) != (j & size))
    corner = jnp.where(pair, below, 0.0).astype(BF16)
    if size == 1:
        return (i == j).astype(BF16) - corner
    inner = bdot(corner, inverse, ((1,), (0,)))
    return inverse - bdot(inverse, inner, ((1,), (0,))).astype(BF16)


def corrected_inverse(below, inverse):
    i = lax.broadcasted_iota(jnp.int32, (ROWS, ROWS), 0)
    j = lax.broadcasted_iota(jnp.int32, (ROWS, ROWS), 1)
    high = below.astype(BF16)
    low = (below - high.astype(F32)).astype(BF16)
    product = bdot(high, inverse, ((1,), (0,))) + bdot(low, inverse, ((1,), (0,)))
    wide = inverse.astype(F32)
    residual = (i == j).astype(F32) - wide - product
    return (wide + bdot(inverse, residual, ((1,), (0,)))).astype(BF16)


def unpack(ref, at):
    body = ref[at].astype(F32)
    return (body[0:192], body[192:193] + body[200:201])


def joined(first, second):
    (body1, a1), (body2, a2) = (first, second)
    turned = bdot(body1, body2[0:128], ((1,), (0,)))
    top = a1 * body2[0:128] + a2 * body1[0:128] - turned[0:128]
    bottom = a2 * body1[128:192] - turned[128:192] + body2[128:192]
    return (jnp.concatenate([top, bottom], axis=0), a1 * a2)


def layer_kernel(
    x_hbm, qw, kw, vw, gvw, ggw, odw, ocw, bw_hbm, dw_hbm, gain_hbm, shift_hbm, pace_hbm, jolt_hbm,
    taps_hbm, norm_hbm, head_hbm, out_ref,
    x_ref, mine, bw, dw, gain_ref, shift_ref, pace_ref, jolt_ref, taps_ref, norm_ref, head_ref,
    g1, g2, f_ref, gate_rows, normed, packet_ref, reach_ref, offset_ref, gated_ref,
    parts, landed, passing, entry_ref, conv_ref,
    slab, before, leaving, near, far, parting, halo, stats, line, wide, filtered,
    zs, zr, xs, xr, ds, dr, ys, yr, us, ur, vs, vr,
    ss, sr, ns, nr, fs, fr, es, er, hs, hr, ts, tr, ps, pr, own,
):
    fetches = [(x_hbm, x_ref)]
    fetches += [(ref, mine.at[n]) for n, ref in enumerate((qw, kw, vw, gvw, ggw, odw, ocw))]
    fetches += [(bw_hbm, bw), (dw_hbm, dw), (gain_hbm, gain_ref), (shift_hbm, shift_ref)]
    fetches += [(pace_hbm, pace_ref), (jolt_hbm, jolt_ref), (taps_hbm, taps_ref)]
    fetches += [(norm_hbm, norm_ref), (head_hbm, head_ref)]
    z, x, c, y = place()
    xp, xm = (lax.rem(x + 1, X), lax.rem(x + X - 1, X))
    opp = lax.rem(x + 2, X)
    right, left = ((z, xp, c, y), (z, xm, c, y))
    other = (z, x, 1 - c, y)
    mates = [(z, x, c, lax.rem(y + d, Y)) for d in (2, 1, 3)]

    def on_z(d):
        return (lax.rem(z + d + Z, Z), x, c, y)

    fetched = [pltpu.make_async_copy(*pair, own.at[3 + n]) for n, pair in enumerate(fetches)]
    for copy in fetched:
        copy.start()
    near[...] = jnp.zeros_like(near)
    far[...] = jnp.zeros_like(far)
    greet([on_z(1), on_z(-1), on_z(2), on_z(-2), right, left, other, (z, opp, c, y)] + mates)
    for copy in fetched:
        copy.wait()

    groups = (g1, g2)
    own_rows = (mine.at[0:3], mine.at[3:7])

    def behind(s):
        return lax.rem(z + Z - s, Z)

    def ahead(s):
        return lax.rem(z + s, Z)

    def z_copy(g, src, zi, s, way, to):
        return remote(src, groups[g].at[:, zi, x, c], zs.at[g, s, way], zr.at[g, s, way], to)

    def z_in(g, s, way):
        zi = behind(s) if way == 0 else ahead(s)
        ref = groups[g].at[:, zi, x, c]
        z_copy(g, ref, zi, s, way, right).wait_recv()

    def z_on(g, s, way, d):
        zi = behind(s) if way == 0 else ahead(s)
        src = own_rows[g] if s == 0 else groups[g].at[:, zi, x, c]
        z_copy(g, src, zi, s + d, way, on_z(d if way == 0 else -d)).start()

    def chunk(zi, xi):
        return g1.at[:, zi, xi, c]

    def x_copy(src, zi, xi, s, way, to):
        return remote(src, chunk(zi, xi), xs.at[s, way], xr.at[s, way], to)

    def d_copy(zi, ci, s, way):
        line = g1.at[:, zi, :, ci]
        return remote(line, line, ds.at[s, way], dr.at[s, way], other)

    def spread_p(s, src):
        x_copy(src, behind(s), x, s, 0, right).start()
        x_copy(src, behind(s), x, s, 1, left).start()

    def spread_q(s):
        src = chunk(ahead(s), x)
        x_copy(src, ahead(s), x, s, 2, left).start()
        x_copy(src, ahead(s), x, s, 3, right).start()

    def forward(s, both):
        p = chunk(behind(s), xm)
        x_copy(p, behind(s), xm, s, 0, right).wait_recv()
        x_copy(p, behind(s), xm, s, 4, right).start()
        if both:
            q = chunk(ahead(s), xp)
            x_copy(q, ahead(s), xp, s, 2, left).wait_recv()
            x_copy(q, ahead(s), xp, s, 5, left).start()

    def across(s, both):
        x_copy(chunk(behind(s), xp), behind(s), xp, s, 1, left).wait_recv()
        x_copy(chunk(behind(s), opp), behind(s), opp, s, 4, right).wait_recv()
        d_copy(behind(s), c, s, 0).start()
        if both:
            x_copy(chunk(ahead(s), xm), ahead(s), xm, s, 3, right).wait_recv()
            x_copy(chunk(ahead(s), opp), ahead(s), opp, s, 5, left).wait_recv()
            d_copy(ahead(s), c, s, 1).start()

    for way in (0, 1):
        z_on(0, 0, way, 2)
        z_on(0, 0, way, 1)
    spread_p(0, own_rows[0])
    yp, ym = (lax.rem(y + 1, Y), lax.rem(y + Y - 1, Y))
    facing_y = lax.rem(y + 2, Y)

    def f_half(yi, half):
        return f_ref.at[yi, half * 128 : half * 128 + 128]

    def f_copy(way, half):
        to = (z, x, c, yp if way == 0 else ym)
        src = x_ref.at[half * 128 : half * 128 + 128]
        return remote(src, f_half(y, half), ys.at[way, half], yr.at[way, half], to)

    def f_arrived(way, half):
        line = f_half(ym if way == 0 else yp, half)
        remote(line, line, ys.at[way, half], yr.at[way, half], other).wait_recv()

    def f_pass(way, yi):
        line = f_half(yi, way)
        to = (z, x, c, yp if way == 0 else ym)
        return remote(line, line, ys.at[way, 2], yr.at[way, 2], to)

    for way in (0, 1):
        f_copy(way, way).start()
    for way in (0, 1):
        f_copy(way, 1 - way).start()
    for way in (0, 1):
        z_on(1, 0, way, 2)
        z_on(1, 0, way, 1)
    keeps = [
        pltpu.make_async_copy(own_rows[0], g1.at[:, z, x, c], own.at[0]),
        pltpu.make_async_copy(own_rows[1], g2.at[:, z, x, c], own.at[1]),
        pltpu.make_async_copy(x_ref, f_ref.at[y], own.at[2]),
    ]
    for copy in keeps:
        copy.start()
    for copy in keeps:
        copy.wait()

    def z_round(r):
        s = 2 * r
        z_in(0, s, 0)
        if s < 8:
            z_on(0, s, 0, 2)
            z_on(0, s, 0, 1)
            z_in(0, s, 1)
            if s < 6:
                z_on(0, s, 1, 2)
            z_on(0, s, 1, 1)
        z_in(0, s - 1, 0)
        z_in(0, s - 1, 1)
        spread_p(s, chunk(behind(s), x))
        if s < 8:
            spread_q(s)
        spread_p(s - 1, chunk(behind(s - 1), x))
        spread_q(s - 1)

    def z_round_later(r):
        s = 2 * r
        z_in(1, s, 0)
        if s < 8:
            z_on(1, s, 0, 2)
            z_on(1, s, 0, 1)
            z_in(1, s, 1)
            if s < 6:
                z_on(1, s, 1, 2)
            z_on(1, s, 1, 1)
        z_in(1, s - 1, 0)
        z_in(1, s - 1, 1)

    z_round(1)
    z_round(2)
    z_round_later(1)
    forward(0, False)
    f_arrived(0, 0)
    f_pass(0, ym).start()
    f_arrived(1, 1)
    f_pass(1, yp).start()
    z_round(3)
    z_round_later(2)
    forward(2, True)
    forward(1, True)
    across(0, False)
    z_round(4)
    forward(4, True)
    forward(3, True)
    z_round_later(3)

    def column(n, xi, ci):
        return g2.at[2 * n : 2 * n + 2, :, xi, ci]

    def half_column(n, xi, k):
        return g2.at[2 * n : 2 * n + 2, 8 * k : 8 * k + 8, xi, c]

    def u_copy(n, xi, way, to):
        return remote(column(n, xi, c), column(n, xi, c), us.at[n, way], ur.at[n, way], to)

    def u_half(n, xi, way, to):
        line = half_column(n, xi, way)
        return remote(line, line, us.at[n, 2 + way], ur.at[n, 2 + way], to)

    def v_copy(n, xi, ci, k):
        return remote(column(n, xi, ci), column(n, xi, ci), vs.at[n, k], vr.at[n, k], other)

    def later_open(n):
        u_copy(n, x, 0, right).start()
        u_copy(n, x, 1, left).start()
        v_copy(n, x, c, 0).start()

    def later_turn(n):
        u_copy(n, xm, 0, right).wait_recv()
        u_half(n, xm, 0, right).start()
        u_copy(n, xp, 1, left).wait_recv()
        u_half(n, xp, 1, left).start()
        v_copy(n, xm, c, 1).start()
        v_copy(n, xp, c, 2).start()

    def later_close(n):
        u_half(n, opp, 0, right).wait_recv()
        u_half(n, opp, 1, left).wait_recv()
        v_copy(n, opp, c, 3).start()

    def later_end(n):
        for k, xi in enumerate((x, xm, xp, opp)):
            v_copy(n, xi, 1 - c, k).wait_recv()

    f_arrived(0, 1)
    f_arrived(1, 0)
    for way in (0, 1):
        f_pass(way, facing_y).wait_recv()

    total = jnp.zeros((ROWS, 1), F32)
    for p in range(Y):
        total = total + jnp.sum(f_ref[p].astype(F32), axis=1, keepdims=True)
    mean = total / 2048.0
    total = jnp.zeros((ROWS, 1), F32)
    for p in range(Y):
        total = total + jnp.sum(jnp.square(f_ref[p].astype(F32) - mean), axis=1, keepdims=True)
    scale = lax.rsqrt(total / 2048.0 + 1e-05)
    for p in range(Y):
        normed[:, p * 512 : (p + 1) * 512] = (
            (f_ref[p].astype(F32) - mean) * scale * gain_ref[p]
        ).astype(BF16)
    forward(6, True)
    forward(5, True)
    across(2, True)
    across(1, True)
    forward(8, False)
    forward(7, True)
    across(4, True)
    across(3, True)
    z_round_later(4)
    later_open(0)
    across(6, True)
    across(5, True)
    i = lax.broadcasted_iota(jnp.int32, (V_HEADS, V_HEADS), 0)
    j = lax.broadcasted_iota(jnp.int32, (V_HEADS, V_HEADS), 1)
    eye = (i == j).astype(F32)
    turned_shift = fdot(eye, shift_ref[...], ((1,), (1,)))
    gate_weights = jnp.concatenate([bw[0], bw[1], dw[0], dw[1]], axis=0)
    every_gate = bdot(gate_weights, normed[...], ((1,), (1,)))
    for n in range(4):
        every_head = every_gate[n * V_HEADS : (n + 1) * V_HEADS]
        if n < 2:
            every_head = jax.nn.sigmoid(every_head + turned_shift[:, n : n + 1])
        for k in range(V_HEADS):
            gate_rows[n, k] = every_head[k : k + 1]
    across(8, False)
    across(7, True)
    first = y * 2

    def two_heads(n):
        return jnp.concatenate([gate_rows[n, first], gate_rows[n, first + 1]], axis=0)

    beta = jnp.concatenate([two_heads(0), two_heads(1)], axis=0)
    pre = jnp.concatenate([two_heads(2), two_heads(3)], axis=0)
    soft = jnp.maximum(pre, 0.0) + jnp.log1p(jnp.exp(-jnp.abs(pre)))
    pace = jnp.concatenate([pace_ref[0], pace_ref[1]], axis=0)
    jolt = jnp.concatenate([jolt_ref[0], jolt_ref[1]], axis=0)
    log_decay = -pace * soft + jolt
    upto = triangle(False, False).astype(F32)
    since = triangle(True, False).astype(F32)
    padded = jnp.concatenate([log_decay, jnp.zeros((4, ROWS), F32)], axis=0)
    forth = fdot(padded, upto, ((1,), (0,)))
    back = fdot(padded, since, ((1,), (0,)))
    cumulative = jnp.concatenate([forth[0:2], back[2:4]], axis=0)
    lines = jnp.concatenate([beta, cumulative], axis=0)
    columns = jnp.transpose(lines)

    def d_arrived(s, way):
        d_copy(behind(s) if way == 0 else ahead(s), 1 - c, s, way).wait_recv()

    d_arrived(0, 0)

    @pl.loop(1, 8)
    def _(s):
        d_arrived(s, 0)
        d_arrived(s, 1)

    d_arrived(8, 0)

    def project(ref, n):
        weight = ref[n].reshape(2048, WIDE)
        return bdot(normed[...], weight, ((1,), (0,))).astype(BF16).astype(F32)

    query_all, key_all, value_all = (project(g1, 0), project(g1, 1), project(g1, 2))
    chains = []
    for h in range(2):
        lanes = slice(h * HEAD, (h + 1) * HEAD)
        q = silu(query_all[:, lanes])
        k = silu(key_all[:, lanes])
        k = k * lax.rsqrt(jnp.sum(jnp.square(k), axis=1, keepdims=True) + 1e-06)
        v = value_all[:, lanes]
        kk = bdot(k, k, ((1,), (1,)))
        qk = bdot(q, k, ((1,), (1,)))
        for e in range(2):
            n = e * 2 + h
            b_col = columns[:, n : n + 1]
            c_col = columns[:, 4 + n : 5 + n]
            c_row = cumulative[n : n + 1, :]
            scores, below = mixing_terms(k, q, v, kk, qk, b_col, c_col, c_row, e == 0)
            chains.append((h, e, q, k, v, b_col, c_col, c_row, scores, below))
    inverses = [None] * 4
    size = 1
    while size < ROWS:
        inverses = [grow_inverse(t[9], inv, size) for t, inv in zip(chains, inverses)]
        size = 2 * size
        if size == 16:
            later_turn(0)
    inverses = [corrected_inverse(t[9], inv) for t, inv in zip(chains, inverses)]
    within = [jnp.zeros((ROWS, HEAD), F32)] * 2
    for (h, e, q, k, v, b_col, c_col, c_row, scores, below), inverse in zip(chains, inverses):
        grown = jnp.exp(c_col)
        rhs = jnp.concatenate([v * b_col, k * (b_col * grown)], axis=1)
        both = bdot(inverse, rhs, ((1,), (0,))).astype(BF16)
        read = bdot(scores, both, ((1,), (0,)))
        within[h] = within[h] + read[:, :HEAD]
        reach_ref[e, h] = (q * grown - read[:, HEAD:]).astype(BF16)
        last = c_row[:, ROWS - 1 : ROWS] if e == 0 else c_row[:, 0:1]
        tail = k * jnp.exp(last - c_col)
        maps = bdot(both, tail, ((0,), (0,)))
        whole = jnp.broadcast_to(jnp.exp(last), (8, HEAD))
        high = whole.astype(BF16).astype(F32)
        scalars = jnp.concatenate([high, whole - high], axis=0).astype(BF16)
        for half in range(2):
            n = e * 4 + h * 2 + half
            packet_ref[n, 0:128] = maps[128:256].astype(BF16)
            packet_ref[n, 128:192] = maps[half * 64 : half * 64 + 64].astype(BF16)
            packet_ref[n, 192:208] = scalars
    for h in range(2):
        offset_ref[h] = within[h]

    step = 1 - 2 * c
    owner = c * X + x
    position = z * 8 + x * 2 + c
    spot = x * 2 + c

    def slab_peer(dx, dc):
        return (z, lax.rem(x + dx, X), c if dc == 0 else 1 - c, y)

    offsets = [(dx, dc) for dx in range(X) for dc in range(C) if (dx, dc) != (0, 0)]
    offsets = sorted(offsets, key=lambda o: -(2 if o[0] == 2 else min(o[0], 1)))

    def at_position(s):
        s = lax.rem(s + 128, 128)
        return (s // 8, lax.rem(s // 2, X), lax.rem(s, 2), y)

    following, preceding = (at_position(position + 1), at_position(position - 1))
    slab_copies = []
    for i, (dx, dc) in enumerate(offsets):
        to = slab_peer(dx, dc)
        copy = remote(
            packet_ref.at[to[2] * X + to[1]], slab.at[spot], ss.at[i], sr.at[i], to
        )
        copy.start()
        slab_copies.append(copy)
    slab[spot] = packet_ref[owner]
    later_close(0)
    later_end(0)
    gated_ref[...] = (project(g2, 0) * jax.nn.sigmoid(project(g2, 1))).astype(BF16)
    halo_copies = [
        remote(gated_ref.at[ROWS - 16 : ROWS], halo.at[0], hs.at[0], hr.at[0], following),
        remote(gated_ref.at[0:16], halo.at[1], hs.at[1], hr.at[1], preceding),
    ]
    for copy in halo_copies:
        copy.start()

    for i, (dx, dc) in enumerate(offsets):
        source = slab_peer(X - dx, dc)
        remote(
            packet_ref.at[owner], slab.at[source[1] * 2 + source[2]], ss.at[i], sr.at[i], source
        ).wait_recv()

    def nth(t):
        return jnp.where(c == 0, t, 7 - t)

    later_open(1)
    running = unpack(slab, nth(0))
    for t in range(1, 8):
        before[t, 0:192] = running[0].astype(BF16)
        parting[t] = running[1]
        running = joined(running, unpack(slab, nth(t)))

    def pack(ref, value):
        body, a = value
        high = a.astype(BF16).astype(F32)
        ref[0:192] = body.astype(BF16)
        ref[192:208] = jnp.concatenate(
            [jnp.broadcast_to(high, (8, HEAD)), jnp.broadcast_to(a - high, (8, HEAD))], axis=0
        ).astype(BF16)

    def hop(d):
        return z + step * d

    def inside(d):
        return (hop(d) >= 0) & (hop(d) < Z)

    def z_peer(d):
        return (jnp.clip(hop(d), 0, Z - 1), x, c, y)

    def near_copy(i, d):
        return remote(leaving.at[0], near.at[i], ns.at[i], nr.at[i], z_peer(d))

    def far_copy(i, d):
        return remote(leaving.at[1], far.at[i], fs.at[i], fr.at[i], z_peer(d))

    pack(leaving.at[0], running)
    for i, d in ((2, 3), (1, 2), (0, 1)):

        @pl.when(inside(d))
        def _():
            near_copy(i, d).start()

    wide[16 : 16 + ROWS] = gated_ref[...].astype(F32)
    for copy in halo_copies:
        copy.wait_recv()
    wide[0:16] = halo[0].astype(F32) * (position > 0).astype(F32)
    wide[16 + ROWS : 32 + ROWS] = halo[1].astype(F32) * (position < 127).astype(F32)
    taps = taps_ref[...].astype(F32)

    @pl.loop(0, ROWS // 32)
    def _(r):
        window = wide[pl.ds(pl.multiple_of(r * 32, 32), 64)]
        total = jnp.zeros((32, WIDE), F32)
        for j in range(KERNEL):
            total = total + window[j + 1 : j + 33] * taps[j : j + 1]
        filtered[pl.ds(pl.multiple_of(r * 32, 32), 32)] = total

    ones = jnp.ones((8, WIDE), F32)
    whole = filtered[...]
    line[0:8] = fdot(ones, whole, ((1,), (1,)))
    line[8:16] = fdot(ones, whole * whole, ((1,), (1,)))
    stat_copies = []
    for i, mate in enumerate(mates):
        copy = remote(line, stats.at[i], ts.at[i], tr.at[i], mate)
        copy.start()
        stat_copies.append(copy)

    window = running
    for i, d in ((0, 1), (1, 2), (2, 3)):

        @pl.when(inside(-d))
        def _():
            near_copy(i, d).wait_recv()

        window = joined(unpack(near, i), window)
    pack(leaving.at[1], window)
    reaches = ((2, 9), (1, 5), (3, 13), (0, 1))
    for i, d in reaches:

        @pl.when(inside(d))
        def _():
            far_copy(i, d).start()

    later_turn(1)

    for copy in stat_copies:
        copy.wait_recv()
    summed = line[...] + stats[0] + stats[1] + stats[2]
    spread = jnp.full((8, WIDE), 0.125, F32)
    mean = fdot(summed[0:8], spread, ((0,), (0,))) / CONV_CH
    second = fdot(summed[8:16], spread, ((0,), (0,))) / CONV_CH
    conv_ref[...] = silu(
        (filtered[...] - mean) * lax.rsqrt(second - mean * mean + 1e-05) * norm_ref[...]
    ).astype(BF16)


    @pl.when(inside(-1))
    def _():
        far_copy(0, 1).wait_recv()

    entering = unpack(far, 0)
    for i, d in ((1, 5), (2, 9), (3, 13)):

        @pl.when(inside(-d))
        def _():
            far_copy(i, d).wait_recv()

        entering = joined(unpack(far, i), entering)
    state = entering[0][128:192]
    line_up = [state]
    for t in range(1, 8):
        body = before[t].astype(F32)
        line_up.append(
            parting[t] * state - bdot(state, body[0:128], ((1,), (0,))) + body[128:192]
        )
    for t in range(8):
        slab[nth(t), 0:64] = line_up[t].astype(BF16)
    entry_ref[owner] = slab[spot, 0:64]
    entry_copies = []
    for i, (dx, dc) in enumerate(offsets):
        to = slab_peer(dx, dc)
        copy = remote(
            slab.at[to[1] * 2 + to[2], 0:64], entry_ref.at[owner], es.at[i], er.at[i], to
        )
        copy.start()
        entry_copies.append(copy)
    later_close(1)
    for i, (dx, dc) in enumerate(offsets):
        source = slab_peer(X - dx, dc)
        remote(
            slab.at[0, 0:64], entry_ref.at[source[2] * X + source[1]], es.at[i], er.at[i], source
        ).wait_recv()
    later_end(1)

    heads = []
    for h in range(2):
        o = offset_ref[h]
        for e in range(2):
            at = e * 4 + h * 2
            state = jnp.concatenate([entry_ref[at], entry_ref[at + 1]], axis=0)
            o = o + bdot(reach_ref[e, h], state, ((1,), (1,)))
        scale = lax.rsqrt(jnp.mean(jnp.square(o), axis=1, keepdims=True) + 1e-06)
        heads.append((o * scale * head_ref[...]).astype(BF16))
    delta = jnp.concatenate(heads, axis=1)
    conv = conv_ref[...]
    beside, facing = (y + 1 - 2 * lax.rem(y, 2), 3 - y)
    opposite = lax.rem(y + 2, Y)
    ways = ((beside, facing), (facing, beside))
    def part_copy(n, k, block):
        to = (z, x, c, ways[n][0])
        return remote(parts.at[n, block], landed.at[n, k], ps.at[n, k], pr.at[n, k], to)

    def pass_copy(n):
        to = (z, x, c, ways[n][1])
        return remote(passing.at[n], landed.at[n, 2], ps.at[n, 2], pr.at[n, 2], to)

    for n in range(2):
        a = g2[2].reshape(2048, WIDE)[n * 1024 : (n + 1) * 1024]
        b = g2[3].reshape(2048, WIDE)[n * 1024 : (n + 1) * 1024]
        total = bdot(delta, a, ((1,), (1,))) + bdot(conv, b, ((1,), (1,)))
        for p in range(Y):
            parts[n, p] = total[p * 64 : (p + 1) * 64].astype(BF16)
        part_copy(n, 0, opposite).start()
    for n in range(2):
        part_copy(n, 1, ways[n][0]).start()
    for n in range(2):
        part_copy(n, 0, opposite).wait_recv()
        passing[n] = (parts[n, ways[n][1]].astype(F32) + landed[n, 0].astype(F32)).astype(BF16)
        pass_copy(n).start()
    for n in range(2):
        part_copy(n, 1, y).wait_recv()
        pass_copy(n).wait_recv()
        out_ref[:, n * 1024 : (n + 1) * 1024] = (
            parts[n, y].astype(F32) + landed[n, 1].astype(F32) + landed[n, 2].astype(F32)
        ).astype(BF16)
    for n in range(2):
        part_copy(n, 0, opposite).wait_send()
        part_copy(n, 1, y).wait_send()
        pass_copy(n).wait_send()
    for copy in slab_copies + halo_copies + stat_copies + entry_copies:
        copy.wait_send()
    for i, d in ((0, 1), (1, 2), (2, 3)):

        @pl.when(inside(d))
        def _():
            near_copy(i, d).wait_send()

    for i, d in reaches:

        @pl.when(inside(d))
        def _():
            far_copy(i, d).wait_send()

    def sent(s, both, zed):
        p, q = (chunk(behind(s), x), chunk(ahead(s), x))
        for g in (0, 1) if zed else ():
            for way in (0, 1) if both else (0,):
                ref = groups[g].at[:, behind(s), x, c]
                z_copy(g, ref, behind(s), s, way, right).wait_send()
        for way in (0, 1, 4) + ((2, 3, 5) if both else ()):
            x_copy(p, behind(s), x, s, way, right).wait_send()
        d_copy(behind(s), c, s, 0).wait_send()
        if both:
            d_copy(ahead(s), c, s, 1).wait_send()

    sent(0, False, False)

    @pl.loop(1, 8)
    def _(s):
        sent(s, True, True)

    sent(8, False, True)
    for way in (0, 1):
        f_copy(way, 0).wait_send()
        f_copy(way, 1).wait_send()
        f_pass(way, ym).wait_send()
    for n in range(2):
        u_copy(n, x, 0, right).wait_send()
        u_copy(n, x, 1, left).wait_send()
        u_half(n, xm, 0, right).wait_send()
        u_half(n, xp, 1, left).wait_send()
        for k in range(4):
            v_copy(n, x, c, k).wait_send()


def layer_call(arrays):
    dma = pltpu.SemaphoreType.DMA
    anywhere = pl.BlockSpec(memory_space=pl.ANY)
    vmem = pltpu.VMEM
    return pl.pallas_call(
        layer_kernel,
        out_shape=jax.ShapeDtypeStruct((64, 2048), BF16),
        in_specs=[anywhere] * len(arrays),
        out_specs=VMEM,
        scratch_shapes=[
            vmem((ROWS, 512), BF16), vmem((7, 16, WIDE), BF16),
            vmem((2, V_HEADS, 2048), BF16), vmem((2, V_HEADS, 2048), BF16),
            vmem((Y, 1, 512), F32), vmem((2, V_HEADS), F32), vmem((2, 2, ROWS), F32),
            vmem((2, 2, ROWS), F32), vmem((KERNEL, WIDE), BF16), vmem((1, WIDE), F32),
            vmem((1, HEAD), F32),
            vmem((3, Z, X, C, 16, WIDE), BF16), vmem((4, Z, X, C, 16, WIDE), BF16),
            vmem((Y, ROWS, 512), BF16), vmem((4, V_HEADS, 1, ROWS), F32),
            vmem((ROWS, 2048), BF16),
            vmem((8, PACKET, HEAD), BF16), vmem((2, 2, ROWS, HEAD), BF16),
            vmem((2, ROWS, HEAD), F32), vmem((ROWS, WIDE), BF16),
            vmem((2, Y, 64, 1024), BF16), vmem((2, 3, 64, 1024), BF16), vmem((2, 64, 1024), BF16),
            vmem((8, 64, HEAD), BF16), vmem((ROWS, WIDE), BF16),
            vmem((8, PACKET, HEAD), BF16), vmem((8, PACKET, HEAD), BF16),
            vmem((2, PACKET, HEAD), BF16), vmem((3, PACKET, HEAD), BF16),
            vmem((4, PACKET, HEAD), BF16), vmem((8, 1, HEAD), F32), vmem((2, 16, WIDE), BF16),
            vmem((3, 16, WIDE), F32), vmem((16, WIDE), F32), vmem((ROWS + 64, WIDE), F32),
            vmem((ROWS, WIDE), F32),
            dma((2, 9, 2)), dma((2, 9, 2)), dma((9, 6)), dma((9, 6)), dma((9, 2)), dma((9, 2)),
            dma((2, 3)), dma((2, 3)), dma((2, 4)), dma((2, 4)), dma((2, 4)), dma((2, 4)),
            dma((7,)), dma((7,)), dma((3,)), dma((3,)), dma((4,)), dma((4,)),
            dma((7,)), dma((7,)), dma((2,)), dma((2,)), dma((3,)), dma((3,)),
            dma((2, 3)), dma((2, 3)), dma((3 + len(arrays),)),
        ],
        compiler_params=pltpu.CompilerParams(
            collective_id=0, has_side_effects=True, vmem_limit_bytes=63 * 2**20
        ),
        name="layer",
    )(*arrays)


def on_device(
    inputs,
    in_gain,
    query_weight,
    key_weight,
    value_weight,
    beta_weight,
    decay_weight,
    beta_shift,
    decay_pace,
    decay_jolt,
    head_gain,
    glu_value_weight,
    glu_gate_weight,
    conv_kernel,
    conv_gain,
    out_delta_weight,
    out_conv_weight,
):
    return layer_call(
        [
            inputs,
            query_weight,
            key_weight,
            value_weight,
            glu_value_weight,
            glu_gate_weight,
            out_delta_weight.T,
            out_conv_weight.T,
            jnp.transpose(beta_weight, (0, 2, 1)),
            jnp.transpose(decay_weight, (0, 2, 1)),
            in_gain.reshape(Y, 1, 512),
            beta_shift,
            decay_pace,
            decay_jolt,
            conv_kernel,
            conv_gain.reshape(1, WIDE),
            head_gain.reshape(1, HEAD),
        ]
    )


def solution(mesh):
    finer = Mesh(mesh.devices.reshape(16, 4, 2, mesh.shape["tp"]), SP_TP)
    in_specs = (
        P(SP, "tp"),
        P(),
        P(SP, "tp"),
        P(SP, "tp"),
        P(SP, "tp"),
        P(),
        P(),
        P(),
        P(None, "tp", SP),
        P(None, "tp", SP),
        P(),
        P(SP, "tp"),
        P(SP, "tp"),
        P(None, "tp"),
        P("tp"),
        P("tp", SP),
        P("tp", SP),
    )
    return jax.shard_map(
        on_device, mesh=finer, in_specs=in_specs, out_specs=P(SP_TP, None), check_vma=False
    )
```

```python
import jax
import jax.numpy as jnp
from jax import lax
from jax.experimental import pallas as pl
from jax.experimental.pallas import tpu as pltpu
from jax.sharding import Mesh
from jax.sharding import PartitionSpec as P

HEAD = 128
V_HEADS = 8
CONV_CH = 1024
KERNEL = 31
SP = ("sp_0", "sp_1", "sp_2")
SP_TP = ("sp_0", "sp_1", "sp_2", "tp")
Z, X, C, Y = (16, 4, 2, 4)
ROWS = 256
WIDE = 256
F32 = jnp.float32
BF16 = jnp.bfloat16
HIGHEST = lax.Precision.HIGHEST
MESH = pl.DeviceIdType.MESH
VMEM = pl.BlockSpec(memory_space=pltpu.VMEM)
PACKET = 208


def place():
    return tuple(lax.axis_index(a) for a in SP_TP)


def remote(src, dst, send, recv, to):
    return pltpu.make_async_remote_copy(
        src_ref=src, dst_ref=dst, send_sem=send, recv_sem=recv, device_id=to, device_id_type=MESH
    )


def greet(peers):
    barrier = pltpu.get_barrier_semaphore()
    for peer in peers:
        pl.semaphore_signal(barrier, inc=1, device_id=peer, device_id_type=MESH)
    pl.semaphore_wait(barrier, len(peers))


def bdot(a, b, dims):
    return lax.dot_general(
        a.astype(BF16), b.astype(BF16), (dims, ((), ())), preferred_element_type=F32
    )


def fdot(a, b, dims):
    return lax.dot_general(a, b, (dims, ((), ())), precision=HIGHEST, preferred_element_type=F32)


def triangle(lower, strict):
    i = lax.broadcasted_iota(jnp.int32, (ROWS, ROWS), 0)
    j = lax.broadcasted_iota(jnp.int32, (ROWS, ROWS), 1)
    if lower:
        return i > j if strict else i >= j
    return i < j if strict else i <= j


def silu(v):
    return v * jax.nn.sigmoid(v)


def mixing_terms(k, q, v, kk, qk, b_col, c_col, c_row, lower):
    mask = triangle(lower, False)
    gap = jnp.where(mask, jnp.exp(jnp.where(mask, c_col - c_row, 0.0)), 0.0)
    below = jnp.where(triangle(lower, True), b_col * kk * gap, 0.0)
    return (qk * gap).astype(BF16), below


def grow_inverse(below, inverse, size):
    i = lax.broadcasted_iota(jnp.int32, (ROWS, ROWS), 0)
    j = lax.broadcasted_iota(jnp.int32, (ROWS, ROWS), 1)
    twice = 2 * size
    pair = ((i & -twice) == (j & -twice)) & ((i & size) != (j & size))
    corner = jnp.where(pair, below, 0.0).astype(BF16)
    if size == 1:
        return (i == j).astype(BF16) - corner
    inner = bdot(corner, inverse, ((1,), (0,)))
    return inverse - bdot(inverse, inner, ((1,), (0,))).astype(BF16)


def corrected_inverse(below, inverse):
    i = lax.broadcasted_iota(jnp.int32, (ROWS, ROWS), 0)
    j = lax.broadcasted_iota(jnp.int32, (ROWS, ROWS), 1)
    high = below.astype(BF16)
    low = (below - high.astype(F32)).astype(BF16)
    product = bdot(high, inverse, ((1,), (0,))) + bdot(low, inverse, ((1,), (0,)))
    wide = inverse.astype(F32)
    residual = (i == j).astype(F32) - wide - product
    return (wide + bdot(inverse, residual, ((1,), (0,)))).astype(BF16)


def unpack(ref, at):
    body = ref[at].astype(F32)
    return (body[0:192], body[192:193] + body[200:201])


def joined(first, second):
    (body1, a1), (body2, a2) = (first, second)
    turned = bdot(body1, body2[0:128], ((1,), (0,)))
    top = a1 * body2[0:128] + a2 * body1[0:128] - turned[0:128]
    bottom = a2 * body1[128:192] - turned[128:192] + body2[128:192]
    return (jnp.concatenate([top, bottom], axis=0), a1 * a2)


def layer_kernel(
    x_hbm, qw, kw, vw, gvw, ggw, odw, ocw, bw_hbm, dw_hbm, gain_hbm, shift_hbm, pace_hbm, jolt_hbm,
    taps_hbm, norm_hbm, head_hbm, out_ref,
    x_ref, mine, bw, dw, gain_ref, shift_ref, pace_ref, jolt_ref, taps_ref, norm_ref, head_ref,
    g1, g2, f_ref, gate_rows, normed, packet_ref, reach_ref, offset_ref, gated_ref,
    parts, landed, passing, entry_ref, conv_ref,
    slab, before, leaving, near, far, parting, halo, stats, line, wide, filtered,
    zs, zr, xs, xr, ds, dr, ys, yr, us, ur, vs, vr,
    ss, sr, ns, nr, fs, fr, es, er, hs, hr, ts, tr, ps, pr, own,
):
    fetches = [(x_hbm, x_ref)]
    fetches += [(ref, mine.at[n]) for n, ref in enumerate((qw, kw, vw, gvw, ggw, odw, ocw))]
    fetches += [(bw_hbm, bw), (dw_hbm, dw), (gain_hbm, gain_ref), (shift_hbm, shift_ref)]
    fetches += [(pace_hbm, pace_ref), (jolt_hbm, jolt_ref), (taps_hbm, taps_ref)]
    fetches += [(norm_hbm, norm_ref), (head_hbm, head_ref)]
    z, x, c, y = place()
    xp, xm = (lax.rem(x + 1, X), lax.rem(x + X - 1, X))
    opp = lax.rem(x + 2, X)
    right, left = ((z, xp, c, y), (z, xm, c, y))
    other = (z, x, 1 - c, y)
    mates = [(z, x, c, lax.rem(y + d, Y)) for d in (2, 1, 3)]

    def on_z(d):
        return (lax.rem(z + d + Z, Z), x, c, y)

    fetched = [pltpu.make_async_copy(*pair, own.at[4 + n]) for n, pair in enumerate(fetches)]
    for copy in fetched:
        copy.start()
    near[...] = jnp.zeros_like(near)
    far[...] = jnp.zeros_like(far)
    greet([on_z(1), on_z(-1), on_z(2), on_z(-2), right, left, other, (z, opp, c, y)] + mates)
    for copy in fetched:
        copy.wait()

    groups = (g1, g2.at[0:2], g2.at[2:4])
    own_rows = (mine.at[0:3], mine.at[3:5], mine.at[5:7])

    def behind(s):
        return lax.rem(z + Z - s, Z)

    def ahead(s):
        return lax.rem(z + s, Z)

    def z_copy(g, src, zi, s, way, to):
        return remote(src, groups[g].at[:, zi, x, c], zs.at[g, s, way], zr.at[g, s, way], to)

    def z_in(g, s, way):
        zi = behind(s) if way == 0 else ahead(s)
        ref = groups[g].at[:, zi, x, c]
        z_copy(g, ref, zi, s, way, right).wait_recv()

    def z_on(g, s, way, d):
        zi = behind(s) if way == 0 else ahead(s)
        src = own_rows[g] if s == 0 else groups[g].at[:, zi, x, c]
        z_copy(g, src, zi, s + d, way, on_z(d if way == 0 else -d)).start()

    def chunk(zi, xi):
        return g1.at[:, zi, xi, c]

    def x_copy(src, zi, xi, s, way, to):
        return remote(src, chunk(zi, xi), xs.at[s, way], xr.at[s, way], to)

    def d_copy(zi, ci, s, way):
        line = g1.at[:, zi, :, ci]
        return remote(line, line, ds.at[s, way], dr.at[s, way], other)

    def spread_p(s, src):
        x_copy(src, behind(s), x, s, 0, right).start()
        x_copy(src, behind(s), x, s, 1, left).start()

    def spread_q(s):
        src = chunk(ahead(s), x)
        x_copy(src, ahead(s), x, s, 2, left).start()
        x_copy(src, ahead(s), x, s, 3, right).start()

    def forward(s, both):
        p = chunk(behind(s), xm)
        x_copy(p, behind(s), xm, s, 0, right).wait_recv()
        x_copy(p, behind(s), xm, s, 4, right).start()
        if both:
            q = chunk(ahead(s), xp)
            x_copy(q, ahead(s), xp, s, 2, left).wait_recv()
            x_copy(q, ahead(s), xp, s, 5, left).start()

    def across(s, both):
        x_copy(chunk(behind(s), xp), behind(s), xp, s, 1, left).wait_recv()
        x_copy(chunk(behind(s), opp), behind(s), opp, s, 4, right).wait_recv()
        d_copy(behind(s), c, s, 0).start()
        if both:
            x_copy(chunk(ahead(s), xm), ahead(s), xm, s, 3, right).wait_recv()
            x_copy(chunk(ahead(s), opp), ahead(s), opp, s, 5, left).wait_recv()
            d_copy(ahead(s), c, s, 1).start()

    for way in (0, 1):
        z_on(0, 0, way, 2)
        z_on(0, 0, way, 1)
    spread_p(0, own_rows[0])
    yp, ym = (lax.rem(y + 1, Y), lax.rem(y + Y - 1, Y))
    facing_y = lax.rem(y + 2, Y)

    def f_half(yi, half):
        return f_ref.at[yi, half * 128 : half * 128 + 128]

    def f_copy(way, half):
        to = (z, x, c, yp if way == 0 else ym)
        src = x_ref.at[half * 128 : half * 128 + 128]
        return remote(src, f_half(y, half), ys.at[way, half], yr.at[way, half], to)

    def f_arrived(way, half):
        line = f_half(ym if way == 0 else yp, half)
        remote(line, line, ys.at[way, half], yr.at[way, half], other).wait_recv()

    def f_pass(way, yi):
        line = f_half(yi, way)
        to = (z, x, c, yp if way == 0 else ym)
        return remote(line, line, ys.at[way, 2], yr.at[way, 2], to)

    for way in (0, 1):
        f_copy(way, way).start()
    for way in (0, 1):
        f_copy(way, 1 - way).start()
    for way in (0, 1):
        z_on(1, 0, way, 2)
        z_on(1, 0, way, 1)
    keeps = [
        pltpu.make_async_copy(own_rows[0], g1.at[:, z, x, c], own.at[0]),
        pltpu.make_async_copy(own_rows[1], groups[1].at[:, z, x, c], own.at[1]),
        pltpu.make_async_copy(own_rows[2], groups[2].at[:, z, x, c], own.at[3]),
        pltpu.make_async_copy(x_ref, f_ref.at[y], own.at[2]),
    ]
    for copy in keeps:
        copy.start()
    for copy in keeps:
        copy.wait()

    def z_round(r):
        s = 2 * r
        z_in(0, s, 0)
        if s < 8:
            z_on(0, s, 0, 2)
            z_on(0, s, 0, 1)
            z_in(0, s, 1)
            if s < 6:
                z_on(0, s, 1, 2)
            z_on(0, s, 1, 1)
        z_in(0, s - 1, 0)
        z_in(0, s - 1, 1)
        spread_p(s, chunk(behind(s), x))
        if s < 8:
            spread_q(s)
        spread_p(s - 1, chunk(behind(s - 1), x))
        spread_q(s - 1)

    def z_round_later(r, g=1):
        s = 2 * r
        z_in(g, s, 0)
        if s < 8:
            z_on(g, s, 0, 2)
            z_on(g, s, 0, 1)
            z_in(g, s, 1)
            if s < 6:
                z_on(g, s, 1, 2)
            z_on(g, s, 1, 1)
        z_in(g, s - 1, 0)
        z_in(g, s - 1, 1)

    z_round(1)
    z_round(2)
    z_round_later(1)
    forward(0, False)
    f_arrived(0, 0)
    f_pass(0, ym).start()
    f_arrived(1, 1)
    f_pass(1, yp).start()
    z_round(3)
    z_round_later(2)
    forward(2, True)
    forward(1, True)
    across(0, False)
    z_round(4)
    forward(4, True)
    forward(3, True)
    z_round_later(3)
    for way in (0, 1):
        z_on(2, 0, way, 2)
        z_on(2, 0, way, 1)

    def column(n, xi, ci):
        return g2.at[2 * n : 2 * n + 2, :, xi, ci]

    def half_column(n, xi, k):
        return g2.at[2 * n : 2 * n + 2, 8 * k : 8 * k + 8, xi, c]

    def u_copy(n, xi, way, to):
        return remote(column(n, xi, c), column(n, xi, c), us.at[n, way], ur.at[n, way], to)

    def u_half(n, xi, way, to):
        line = half_column(n, xi, way)
        return remote(line, line, us.at[n, 2 + way], ur.at[n, 2 + way], to)

    def v_copy(n, xi, ci, k):
        return remote(column(n, xi, ci), column(n, xi, ci), vs.at[n, k], vr.at[n, k], other)

    def later_open(n):
        u_copy(n, x, 0, right).start()
        u_copy(n, x, 1, left).start()
        v_copy(n, x, c, 0).start()

    def later_turn(n):
        u_copy(n, xm, 0, right).wait_recv()
        u_half(n, xm, 0, right).start()
        u_copy(n, xp, 1, left).wait_recv()
        u_half(n, xp, 1, left).start()
        v_copy(n, xm, c, 1).start()
        v_copy(n, xp, c, 2).start()

    def later_close(n):
        u_half(n, opp, 0, right).wait_recv()
        u_half(n, opp, 1, left).wait_recv()
        v_copy(n, opp, c, 3).start()

    def later_end(n):
        for k, xi in enumerate((x, xm, xp, opp)):
            v_copy(n, xi, 1 - c, k).wait_recv()

    f_arrived(0, 1)
    f_arrived(1, 0)
    for way in (0, 1):
        f_pass(way, facing_y).wait_recv()

    total = jnp.zeros((ROWS, 1), F32)
    for p in range(Y):
        total = total + jnp.sum(f_ref[p].astype(F32), axis=1, keepdims=True)
    mean = total / 2048.0
    total = jnp.zeros((ROWS, 1), F32)
    for p in range(Y):
        total = total + jnp.sum(jnp.square(f_ref[p].astype(F32) - mean), axis=1, keepdims=True)
    scale = lax.rsqrt(total / 2048.0 + 1e-05)
    for p in range(Y):
        normed[:, p * 512 : (p + 1) * 512] = (
            (f_ref[p].astype(F32) - mean) * scale * gain_ref[p]
        ).astype(BF16)
    forward(6, True)
    forward(5, True)
    across(2, True)
    across(1, True)
    forward(8, False)
    forward(7, True)
    across(4, True)
    across(3, True)
    z_round_later(4)
    later_open(0)
    z_round_later(1, 2)
    across(6, True)
    across(5, True)
    i = lax.broadcasted_iota(jnp.int32, (V_HEADS, V_HEADS), 0)
    j = lax.broadcasted_iota(jnp.int32, (V_HEADS, V_HEADS), 1)
    eye = (i == j).astype(F32)
    turned_shift = fdot(eye, shift_ref[...], ((1,), (1,)))
    gate_weights = jnp.concatenate([bw[0], bw[1], dw[0], dw[1]], axis=0)
    every_gate = bdot(gate_weights, normed[...], ((1,), (1,)))
    for n in range(4):
        every_head = every_gate[n * V_HEADS : (n + 1) * V_HEADS]
        if n < 2:
            every_head = jax.nn.sigmoid(every_head + turned_shift[:, n : n + 1])
        for k in range(V_HEADS):
            gate_rows[n, k] = every_head[k : k + 1]
    across(8, False)
    across(7, True)
    first = y * 2

    def two_heads(n):
        return jnp.concatenate([gate_rows[n, first], gate_rows[n, first + 1]], axis=0)

    beta = jnp.concatenate([two_heads(0), two_heads(1)], axis=0)
    pre = jnp.concatenate([two_heads(2), two_heads(3)], axis=0)
    soft = jnp.maximum(pre, 0.0) + jnp.log1p(jnp.exp(-jnp.abs(pre)))
    pace = jnp.concatenate([pace_ref[0], pace_ref[1]], axis=0)
    jolt = jnp.concatenate([jolt_ref[0], jolt_ref[1]], axis=0)
    log_decay = -pace * soft + jolt
    upto = triangle(False, False).astype(F32)
    since = triangle(True, False).astype(F32)
    padded = jnp.concatenate([log_decay, jnp.zeros((4, ROWS), F32)], axis=0)
    forth = fdot(padded, upto, ((1,), (0,)))
    back = fdot(padded, since, ((1,), (0,)))
    cumulative = jnp.concatenate([forth[0:2], back[2:4]], axis=0)
    lines = jnp.concatenate([beta, cumulative], axis=0)
    columns = jnp.transpose(lines)

    def d_arrived(s, way):
        d_copy(behind(s) if way == 0 else ahead(s), 1 - c, s, way).wait_recv()

    d_arrived(0, 0)

    @pl.loop(1, 8)
    def _(s):
        d_arrived(s, 0)
        d_arrived(s, 1)

    d_arrived(8, 0)

    def project(ref, n):
        weight = ref[n].reshape(2048, WIDE)
        return bdot(normed[...], weight, ((1,), (0,))).astype(BF16).astype(F32)

    z_round_later(2, 2)
    query_all, key_all, value_all = (project(g1, 0), project(g1, 1), project(g1, 2))
    chains = []
    for h in range(2):
        lanes = slice(h * HEAD, (h + 1) * HEAD)
        q = silu(query_all[:, lanes])
        k = silu(key_all[:, lanes])
        k = k * lax.rsqrt(jnp.sum(jnp.square(k), axis=1, keepdims=True) + 1e-06)
        v = value_all[:, lanes]
        kk = bdot(k, k, ((1,), (1,)))
        qk = bdot(q, k, ((1,), (1,)))
        for e in range(2):
            n = e * 2 + h
            b_col = columns[:, n : n + 1]
            c_col = columns[:, 4 + n : 5 + n]
            c_row = cumulative[n : n + 1, :]
            scores, below = mixing_terms(k, q, v, kk, qk, b_col, c_col, c_row, e == 0)
            chains.append((h, e, q, k, v, b_col, c_col, c_row, scores, below))
    inverses = [None] * 4
    size = 1
    while size < ROWS:
        inverses = [grow_inverse(t[9], inv, size) for t, inv in zip(chains, inverses)]
        size = 2 * size
        if size == 16:
            later_turn(0)
            z_round_later(3, 2)
    inverses = [corrected_inverse(t[9], inv) for t, inv in zip(chains, inverses)]
    within = [jnp.zeros((ROWS, HEAD), F32)] * 2
    for (h, e, q, k, v, b_col, c_col, c_row, scores, below), inverse in zip(chains, inverses):
        grown = jnp.exp(c_col)
        rhs = jnp.concatenate([v * b_col, k * (b_col * grown)], axis=1)
        both = bdot(inverse, rhs, ((1,), (0,))).astype(BF16)
        read = bdot(scores, both, ((1,), (0,)))
        within[h] = within[h] + read[:, :HEAD]
        reach_ref[e, h] = (q * grown - read[:, HEAD:]).astype(BF16)
        last = c_row[:, ROWS - 1 : ROWS] if e == 0 else c_row[:, 0:1]
        tail = k * jnp.exp(last - c_col)
        maps = bdot(both, tail, ((0,), (0,)))
        whole = jnp.broadcast_to(jnp.exp(last), (8, HEAD))
        high = whole.astype(BF16).astype(F32)
        scalars = jnp.concatenate([high, whole - high], axis=0).astype(BF16)
        for half in range(2):
            n = e * 4 + h * 2 + half
            packet_ref[n, 0:128] = maps[128:256].astype(BF16)
            packet_ref[n, 128:192] = maps[half * 64 : half * 64 + 64].astype(BF16)
            packet_ref[n, 192:208] = scalars
    for h in range(2):
        offset_ref[h] = within[h]

    step = 1 - 2 * c
    owner = c * X + x
    position = z * 8 + x * 2 + c
    spot = x * 2 + c

    def slab_peer(dx, dc):
        return (z, lax.rem(x + dx, X), c if dc == 0 else 1 - c, y)

    offsets = [(dx, dc) for dx in range(X) for dc in range(C) if (dx, dc) != (0, 0)]
    offsets = sorted(offsets, key=lambda o: -(2 if o[0] == 2 else min(o[0], 1)))

    def at_position(s):
        s = lax.rem(s + 128, 128)
        return (s // 8, lax.rem(s // 2, X), lax.rem(s, 2), y)

    following, preceding = (at_position(position + 1), at_position(position - 1))
    slab_copies = []
    for i, (dx, dc) in enumerate(offsets):
        to = slab_peer(dx, dc)
        copy = remote(
            packet_ref.at[to[2] * X + to[1]], slab.at[spot], ss.at[i], sr.at[i], to
        )
        copy.start()
        slab_copies.append(copy)
    slab[spot] = packet_ref[owner]
    z_round_later(4, 2)
    later_close(0)
    later_end(0)
    gated_ref[...] = (project(g2, 0) * jax.nn.sigmoid(project(g2, 1))).astype(BF16)
    halo_copies = [
        remote(gated_ref.at[ROWS - 16 : ROWS], halo.at[0], hs.at[0], hr.at[0], following),
        remote(gated_ref.at[0:16], halo.at[1], hs.at[1], hr.at[1], preceding),
    ]
    for copy in halo_copies:
        copy.start()

    for i, (dx, dc) in enumerate(offsets):
        source = slab_peer(X - dx, dc)
        remote(
            packet_ref.at[owner], slab.at[source[1] * 2 + source[2]], ss.at[i], sr.at[i], source
        ).wait_recv()

    def nth(t):
        return jnp.where(c == 0, t, 7 - t)

    later_open(1)
    running = unpack(slab, nth(0))
    for t in range(1, 8):
        before[t, 0:192] = running[0].astype(BF16)
        parting[t] = running[1]
        running = joined(running, unpack(slab, nth(t)))

    def pack(ref, value):
        body, a = value
        high = a.astype(BF16).astype(F32)
        ref[0:192] = body.astype(BF16)
        ref[192:208] = jnp.concatenate(
            [jnp.broadcast_to(high, (8, HEAD)), jnp.broadcast_to(a - high, (8, HEAD))], axis=0
        ).astype(BF16)

    def hop(d):
        return z + step * d

    def inside(d):
        return (hop(d) >= 0) & (hop(d) < Z)

    def z_peer(d):
        return (jnp.clip(hop(d), 0, Z - 1), x, c, y)

    def near_copy(i, d):
        return remote(leaving.at[0], near.at[i], ns.at[i], nr.at[i], z_peer(d))

    def far_copy(i, d):
        return remote(leaving.at[1], far.at[i], fs.at[i], fr.at[i], z_peer(d))

    pack(leaving.at[0], running)
    for i, d in ((2, 3), (1, 2), (0, 1)):

        @pl.when(inside(d))
        def _():
            near_copy(i, d).start()

    wide[16 : 16 + ROWS] = gated_ref[...].astype(F32)
    for copy in halo_copies:
        copy.wait_recv()
    wide[0:16] = halo[0].astype(F32) * (position > 0).astype(F32)
    wide[16 + ROWS : 32 + ROWS] = halo[1].astype(F32) * (position < 127).astype(F32)
    taps = taps_ref[...].astype(F32)

    @pl.loop(0, ROWS // 32)
    def _(r):
        window = wide[pl.ds(pl.multiple_of(r * 32, 32), 64)]
        total = jnp.zeros((32, WIDE), F32)
        for j in range(KERNEL):
            total = total + window[j + 1 : j + 33] * taps[j : j + 1]
        filtered[pl.ds(pl.multiple_of(r * 32, 32), 32)] = total

    ones = jnp.ones((8, WIDE), F32)
    whole = filtered[...]
    line[0:8] = fdot(ones, whole, ((1,), (1,)))
    line[8:16] = fdot(ones, whole * whole, ((1,), (1,)))
    stat_copies = []
    for i, mate in enumerate(mates):
        copy = remote(line, stats.at[i], ts.at[i], tr.at[i], mate)
        copy.start()
        stat_copies.append(copy)

    window = running
    for i, d in ((0, 1), (1, 2), (2, 3)):

        @pl.when(inside(-d))
        def _():
            near_copy(i, d).wait_recv()

        window = joined(unpack(near, i), window)
    pack(leaving.at[1], window)
    reaches = ((2, 9), (1, 5), (3, 13), (0, 1))
    for i, d in reaches:

        @pl.when(inside(d))
        def _():
            far_copy(i, d).start()

    later_turn(1)

    for copy in stat_copies:
        copy.wait_recv()
    summed = line[...] + stats[0] + stats[1] + stats[2]
    spread = jnp.full((8, WIDE), 0.125, F32)
    mean = fdot(summed[0:8], spread, ((0,), (0,))) / CONV_CH
    second = fdot(summed[8:16], spread, ((0,), (0,))) / CONV_CH
    conv_ref[...] = silu(
        (filtered[...] - mean) * lax.rsqrt(second - mean * mean + 1e-05) * norm_ref[...]
    ).astype(BF16)


    @pl.when(inside(-1))
    def _():
        far_copy(0, 1).wait_recv()

    entering = unpack(far, 0)
    for i, d in ((1, 5), (2, 9), (3, 13)):

        @pl.when(inside(-d))
        def _():
            far_copy(i, d).wait_recv()

        entering = joined(unpack(far, i), entering)
    state = entering[0][128:192]
    line_up = [state]
    for t in range(1, 8):
        body = before[t].astype(F32)
        line_up.append(
            parting[t] * state - bdot(state, body[0:128], ((1,), (0,))) + body[128:192]
        )
    for t in range(8):
        slab[nth(t), 0:64] = line_up[t].astype(BF16)
    entry_ref[owner] = slab[spot, 0:64]
    entry_copies = []
    for i, (dx, dc) in enumerate(offsets):
        to = slab_peer(dx, dc)
        copy = remote(
            slab.at[to[1] * 2 + to[2], 0:64], entry_ref.at[owner], es.at[i], er.at[i], to
        )
        copy.start()
        entry_copies.append(copy)
    later_close(1)
    for i, (dx, dc) in enumerate(offsets):
        source = slab_peer(X - dx, dc)
        remote(
            slab.at[0, 0:64], entry_ref.at[source[2] * X + source[1]], es.at[i], er.at[i], source
        ).wait_recv()
    later_end(1)

    heads = []
    for h in range(2):
        o = offset_ref[h]
        for e in range(2):
            at = e * 4 + h * 2
            state = jnp.concatenate([entry_ref[at], entry_ref[at + 1]], axis=0)
            o = o + bdot(reach_ref[e, h], state, ((1,), (1,)))
        scale = lax.rsqrt(jnp.mean(jnp.square(o), axis=1, keepdims=True) + 1e-06)
        heads.append((o * scale * head_ref[...]).astype(BF16))
    delta = jnp.concatenate(heads, axis=1)
    conv = conv_ref[...]
    beside, facing = (y + 1 - 2 * lax.rem(y, 2), 3 - y)
    opposite = lax.rem(y + 2, Y)
    ways = ((beside, facing), (facing, beside))
    def part_copy(n, k, block):
        to = (z, x, c, ways[n][0])
        return remote(parts.at[n, block], landed.at[n, k], ps.at[n, k], pr.at[n, k], to)

    def pass_copy(n):
        to = (z, x, c, ways[n][1])
        return remote(passing.at[n], landed.at[n, 2], ps.at[n, 2], pr.at[n, 2], to)

    for n in range(2):
        a = g2[2].reshape(2048, WIDE)[n * 1024 : (n + 1) * 1024]
        b = g2[3].reshape(2048, WIDE)[n * 1024 : (n + 1) * 1024]
        total = bdot(delta, a, ((1,), (1,))) + bdot(conv, b, ((1,), (1,)))
        for p in range(Y):
            parts[n, p] = total[p * 64 : (p + 1) * 64].astype(BF16)
        part_copy(n, 0, opposite).start()
    for n in range(2):
        part_copy(n, 1, ways[n][0]).start()
    for n in range(2):
        part_copy(n, 0, opposite).wait_recv()
        passing[n] = (parts[n, ways[n][1]].astype(F32) + landed[n, 0].astype(F32)).astype(BF16)
        pass_copy(n).start()
    for n in range(2):
        part_copy(n, 1, y).wait_recv()
        pass_copy(n).wait_recv()
        out_ref[:, n * 1024 : (n + 1) * 1024] = (
            parts[n, y].astype(F32) + landed[n, 1].astype(F32) + landed[n, 2].astype(F32)
        ).astype(BF16)
    for n in range(2):
        part_copy(n, 0, opposite).wait_send()
        part_copy(n, 1, y).wait_send()
        pass_copy(n).wait_send()
    for copy in slab_copies + halo_copies + stat_copies + entry_copies:
        copy.wait_send()
    for i, d in ((0, 1), (1, 2), (2, 3)):

        @pl.when(inside(d))
        def _():
            near_copy(i, d).wait_send()

    for i, d in reaches:

        @pl.when(inside(d))
        def _():
            far_copy(i, d).wait_send()

    def sent(s, both, zed):
        p, q = (chunk(behind(s), x), chunk(ahead(s), x))
        for g in (0, 1, 2) if zed else ():
            for way in (0, 1) if both else (0,):
                ref = groups[g].at[:, behind(s), x, c]
                z_copy(g, ref, behind(s), s, way, right).wait_send()
        for way in (0, 1, 4) + ((2, 3, 5) if both else ()):
            x_copy(p, behind(s), x, s, way, right).wait_send()
        d_copy(behind(s), c, s, 0).wait_send()
        if both:
            d_copy(ahead(s), c, s, 1).wait_send()

    sent(0, False, False)

    @pl.loop(1, 8)
    def _(s):
        sent(s, True, True)

    sent(8, False, True)
    for way in (0, 1):
        f_copy(way, 0).wait_send()
        f_copy(way, 1).wait_send()
        f_pass(way, ym).wait_send()
    for n in range(2):
        u_copy(n, x, 0, right).wait_send()
        u_copy(n, x, 1, left).wait_send()
        u_half(n, xm, 0, right).wait_send()
        u_half(n, xp, 1, left).wait_send()
        for k in range(4):
            v_copy(n, x, c, k).wait_send()


def layer_call(arrays):
    dma = pltpu.SemaphoreType.DMA
    anywhere = pl.BlockSpec(memory_space=pl.ANY)
    vmem = pltpu.VMEM
    return pl.pallas_call(
        layer_kernel,
        out_shape=jax.ShapeDtypeStruct((64, 2048), BF16),
        in_specs=[anywhere] * len(arrays),
        out_specs=VMEM,
        scratch_shapes=[
            vmem((ROWS, 512), BF16), vmem((7, 16, WIDE), BF16),
            vmem((2, V_HEADS, 2048), BF16), vmem((2, V_HEADS, 2048), BF16),
            vmem((Y, 1, 512), F32), vmem((2, V_HEADS), F32), vmem((2, 2, ROWS), F32),
            vmem((2, 2, ROWS), F32), vmem((KERNEL, WIDE), BF16), vmem((1, WIDE), F32),
            vmem((1, HEAD), F32),
            vmem((3, Z, X, C, 16, WIDE), BF16), vmem((4, Z, X, C, 16, WIDE), BF16),
            vmem((Y, ROWS, 512), BF16), vmem((4, V_HEADS, 1, ROWS), F32),
            vmem((ROWS, 2048), BF16),
            vmem((8, PACKET, HEAD), BF16), vmem((2, 2, ROWS, HEAD), BF16),
            vmem((2, ROWS, HEAD), F32), vmem((ROWS, WIDE), BF16),
            vmem((2, Y, 64, 1024), BF16), vmem((2, 3, 64, 1024), BF16), vmem((2, 64, 1024), BF16),
            vmem((8, 64, HEAD), BF16), vmem((ROWS, WIDE), BF16),
            vmem((8, PACKET, HEAD), BF16), vmem((8, PACKET, HEAD), BF16),
            vmem((2, PACKET, HEAD), BF16), vmem((3, PACKET, HEAD), BF16),
            vmem((4, PACKET, HEAD), BF16), vmem((8, 1, HEAD), F32), vmem((2, 16, WIDE), BF16),
            vmem((3, 16, WIDE), F32), vmem((16, WIDE), F32), vmem((ROWS + 64, WIDE), F32),
            vmem((ROWS, WIDE), F32),
            dma((3, 9, 2)), dma((3, 9, 2)), dma((9, 6)), dma((9, 6)), dma((9, 2)), dma((9, 2)),
            dma((2, 3)), dma((2, 3)), dma((2, 4)), dma((2, 4)), dma((2, 4)), dma((2, 4)),
            dma((7,)), dma((7,)), dma((3,)), dma((3,)), dma((4,)), dma((4,)),
            dma((7,)), dma((7,)), dma((2,)), dma((2,)), dma((3,)), dma((3,)),
            dma((2, 3)), dma((2, 3)), dma((4 + len(arrays),)),
        ],
        compiler_params=pltpu.CompilerParams(
            collective_id=0, has_side_effects=True, vmem_limit_bytes=63 * 2**20
        ),
        name="layer",
    )(*arrays)


def on_device(
    inputs,
    in_gain,
    query_weight,
    key_weight,
    value_weight,
    beta_weight,
    decay_weight,
    beta_shift,
    decay_pace,
    decay_jolt,
    head_gain,
    glu_value_weight,
    glu_gate_weight,
    conv_kernel,
    conv_gain,
    out_delta_weight,
    out_conv_weight,
):
    return layer_call(
        [
            inputs,
            query_weight,
            key_weight,
            value_weight,
            glu_value_weight,
            glu_gate_weight,
            out_delta_weight.T,
            out_conv_weight.T,
            jnp.transpose(beta_weight, (0, 2, 1)),
            jnp.transpose(decay_weight, (0, 2, 1)),
            in_gain.reshape(Y, 1, 512),
            beta_shift,
            decay_pace,
            decay_jolt,
            conv_kernel,
            conv_gain.reshape(1, WIDE),
            head_gain.reshape(1, HEAD),
        ]
    )


def solution(mesh):
    finer = Mesh(mesh.devices.reshape(16, 4, 2, mesh.shape["tp"]), SP_TP)
    in_specs = (
        P(SP, "tp"),
        P(),
        P(SP, "tp"),
        P(SP, "tp"),
        P(SP, "tp"),
        P(),
        P(),
        P(),
        P(None, "tp", SP),
        P(None, "tp", SP),
        P(),
        P(SP, "tp"),
        P(SP, "tp"),
        P(None, "tp"),
        P("tp"),
        P("tp", SP),
        P("tp", SP),
    )
    return jax.shard_map(
        on_device, mesh=finer, in_specs=in_specs, out_specs=P(SP_TP, None), check_vma=False
    )
```
